512 devices in a mesh: sp: 64 (over z, y), tp: 8 (over x, core).
Axes of the slice: x: 4, y: 4, z: 16, core: 2. Of those that a mesh axis runs over, the one named last changes fastest.
Arguments:
- skip_stream_entering: bfloat16 [8192, 2048], P(('sp', 'tp')), may hold values from -6 to 6
- content_signal_matrix: bfloat16 [8192, 4096], P('sp', 'tp'), may hold values from -6 to 6
- writer_signal_matrix: bfloat16 [8192, 1024], P('sp', 'tp'), may hold values from -6 to 6
- reader_signal_matrix: bfloat16 [8192, 1024], P('sp', 'tp'), may hold values from -6 to 6
- multiplier_signal: bfloat16 [8192, 4096], P('sp', 'tp'), may hold values from -6 to 6
- interval_before_softplus: float32 [64, 8192], P('tp', 'sp'), may hold values from -7.5 to 0.5
- extra_log_shrink: float32 [64, 8192], P('tp', 'sp'), may hold values from -2.8 to 0
- log_forget_speed: float32 [64], P('tp'), may hold values from -12 to 0
- content_filter_coefs: bfloat16 [4, 4096], P(None, 'tp'), may hold values from -3 to 3
- writer_filter_coefs: bfloat16 [4, 1024], P(None, 'tp'), may hold values from -3 to 3
- reader_filter_coefs: bfloat16 [4, 1024], P(None, 'tp'), may hold values from -3 to 3
- skip_path_factor: float32 [64], P('tp'), may hold values from 0.25 to 2
- cluster_scaling_vector: float32 [4096], P('tp'), may hold values from 0.1 to 1.9
- blend_result_matrix: bfloat16 [4096, 2048], P('tp'), may hold values from -0.09375 to 0.09375
- feature_blend_scaling: float32 [2048], replicated, may hold values from 0.1 to 1.9
- widening_matrix: bfloat16 [2048, 8192], P('sp', 'tp'), may hold values from -0.125 to 0.125
- narrowing_matrix: bfloat16 [8192, 2048], P('tp', 'sp'), may hold values from -0.0625 to 0.0625
Outputs:
- layer_out: bfloat16 [8192, 2048], P(('sp', 'tp'))
The draws below stay inside these ranges and needn't reach their ends.
All inputs are finite; a program needn't handle non-finite values.
Results may differ from the reference program's by a relative error of at most 0.02.
Values may be sent and summed in bfloat16 or wider, within the bound.
No kernel may reach another device: no remote copies, remote signals or barrier semaphores. Data moves between devices by JAX's collectives and lax.ppermute only.
A program may use at most 64 MiB of HBM per device.

```python
import math
import jax
import jax.numpy as jnp
from jax import lax

D = 2048
HEADS = 64
HEAD_DIM = 64
GROUPS = 8
STATE = 128
FF = 8192
CONV = 4
BLOCK = 128
TOK_DEV = 128
D_INNER = 4096
TOKENS = 8192
N_TP = 8


def draw_interval_before_softplus(key, part):
    noise_key, shift_key = jax.random.split(jax.random.fold_in(key, 11))
    noise = jnp.clip(jax.random.normal(noise_key, (HEADS, TOKENS), jnp.float32), -3.0, 3.0)
    offsets = jax.random.uniform(shift_key, (TOKENS // TOK_DEV,), jnp.float32, -1.0, 1.0)
    return -3.5 + noise + jnp.repeat(offsets, TOK_DEV)[None, :]


def draw_log_forget_speed(key, part):
    order_key, slow_key, fast_key = jax.random.split(jax.random.fold_in(key, 23), 3)
    order = jax.random.permutation(order_key, HEADS)
    slow = order < HEADS // 2
    slow_rate = jnp.exp(jax.random.uniform(slow_key, (HEADS,), jnp.float32, math.log(0.3), 0.0)) / (0.06 * TOKENS)
    fast_rate = jnp.exp(jax.random.uniform(fast_key, (HEADS,), jnp.float32, math.log(0.17), math.log(0.55)))
    return jnp.log(jnp.where(slow, slow_rate, fast_rate))


def draw_extra_log_shrink(key, part):
    where_key, depth_key = jax.random.split(jax.random.fold_in(key, 37))
    places = jax.random.randint(where_key, (4,), 0, TOKENS)
    depths = jax.random.uniform(depth_key, (HEADS, 4), jnp.float32, math.log(0.5), math.log(0.8))
    indicator = (jnp.arange(TOKENS)[None, :] == places[:, None]).astype(jnp.float32)
    return jnp.dot(depths, indicator, precision=lax.Precision.HIGHEST)


def level_of(key, dims, pieces, least, top_value):
    def one(axis_at, parts):
        steps = jax.random.uniform(jax.random.fold_in(jax.random.fold_in(key, 6), axis_at), (parts,), jnp.float32, least / len(pieces), top_value / len(pieces))
        return jnp.repeat(jnp.exp(steps), dims[axis_at] // parts).reshape((-1,) + (1,) * (len(dims) - axis_at - 1))

    factor_of = one(*pieces[0])
    for cut in pieces[1:]:
        factor_of = factor_of * one(*cut)
    return factor_of


def centred(key, extent, spread, limit, pieces=(), kind=jnp.bfloat16):
    values = spread * jax.random.normal(key, extent, jnp.float32)
    if pieces:
        values = values * level_of(key, extent, pieces, -0.22, 0.18)
    return jnp.clip(values, -limit, limit).astype(kind)


def setup_inputs(seed: int = 0) -> dict:
    arg_keys = jax.random.split(jax.random.key(seed), 18)
    return {
        "skip_stream_entering": centred(arg_keys[0], (TOKENS, D), 1.0, 6.0, ((0, 512),)),
        "content_signal_matrix": centred(arg_keys[1], (TOKENS, D_INNER), 1.0, 6.0, ((0, 64), (1, 8))),
        "writer_signal_matrix": centred(arg_keys[2], (TOKENS, GROUPS * STATE), 1.0, 6.0, ((0, 64), (1, 8))),
        "reader_signal_matrix": centred(arg_keys[3], (TOKENS, GROUPS * STATE), 1.0, 6.0, ((0, 64), (1, 8))),
        "multiplier_signal": centred(arg_keys[4], (TOKENS, D_INNER), 1.0, 6.0, ((0, 64), (1, 8))),
        "interval_before_softplus": draw_interval_before_softplus(jax.random.fold_in(arg_keys[17], 71), 0),
        "extra_log_shrink": draw_extra_log_shrink(jax.random.fold_in(arg_keys[17], 71), 0),
        "log_forget_speed": draw_log_forget_speed(jax.random.fold_in(arg_keys[17], 71), 0),
        "content_filter_coefs": centred(arg_keys[8], (CONV, D_INNER), 0.5, 3.0, ((1, 8),)),
        "writer_filter_coefs": centred(arg_keys[9], (CONV, GROUPS * STATE), 0.5, 3.0, ((1, 8),)),
        "reader_filter_coefs": centred(arg_keys[10], (CONV, GROUPS * STATE), 0.5, 3.0, ((1, 8),)),
        "skip_path_factor": jnp.clip(0.25 + 1.75 * jax.random.uniform(arg_keys[11], (HEADS,), jnp.float32) ** level_of(arg_keys[11], (HEADS,), ((0, 8),), -0.2, 0.2), 0.25, 2.0),
        "cluster_scaling_vector": jnp.clip(1.0 + 0.18 * jax.random.normal(arg_keys[12], (D_INNER,), jnp.float32), 0.1, 1.9),
        "blend_result_matrix": centred(arg_keys[13], (D_INNER, D), D_INNER ** -0.5, 0.09375, ((0, 8),)),
        "feature_blend_scaling": jnp.clip(1.0 + 0.18 * jax.random.normal(arg_keys[14], (D,), jnp.float32), 0.1, 1.9),
        "widening_matrix": centred(arg_keys[15], (D, FF), D ** -0.5, 0.125, ((0, 64), (1, 8))),
        "narrowing_matrix": centred(arg_keys[16], (FF, D), FF ** -0.5, 0.0625, ((0, 8), (1, 64))),
    }


epsilon = 1e-05
precise = lax.Precision.HIGHEST

def convolve(inputs, conv_taps):
    width = conv_taps.shape[0]
    length = inputs.shape[0]
    extended = jnp.pad(inputs, ((width - 1, 0), (0, 0)))
    summed = extended[0:length].astype(jnp.float32) * conv_taps[0].astype(jnp.float32)
    for offset in range(1, width):
        summed = summed + extended[offset:offset + length].astype(jnp.float32) * conv_taps[offset].astype(jnp.float32)
    return jax.nn.silu(summed)

def advance(carried, pair):
    block_state, block_factor = pair
    return (carried * block_factor[..., None, None] + block_state, carried)

def blockwise(values, interval_lengths, log_forgetting, key_rows, query_rows):
    length, groups, per_group, width = values.shape
    blocks = length // BLOCK
    value_blocks = values.reshape(blocks, BLOCK, groups, per_group, width)
    step_blocks = jnp.transpose(interval_lengths.reshape(groups, per_group, blocks, BLOCK), (2, 3, 0, 1))
    weighted = value_blocks * step_blocks[..., None]
    cumulative = jnp.cumsum(jnp.transpose(log_forgetting.reshape(groups, per_group, blocks, BLOCK), (2, 0, 1, 3)), axis=-1)
    key_blocks = key_rows.reshape(blocks, BLOCK, groups, -1)
    query_blocks = query_rows.reshape(blocks, BLOCK, groups, -1)
    causal = jnp.tril(jnp.ones((BLOCK, BLOCK), dtype=bool))
    decay_mask = jnp.exp(jnp.where(causal, cumulative[..., :, None] - cumulative[..., None, :], -jnp.inf))
    scores = jnp.einsum('clgn,csgn->cgls', query_blocks, key_blocks, precision=precise)
    within = jnp.einsum('cgls,cgrls,csgrp->clgrp', scores, decay_mask, weighted, precision=precise)
    to_end = jnp.exp(cumulative[..., -1:] - cumulative)
    states = jnp.einsum('clgn,cgrl,clgrp->cgrpn', key_blocks, to_end, weighted, precision=precise)
    block_totals = cumulative[..., -1]
    initial = jnp.zeros(states.shape[1:], jnp.float32)
    final, entering = lax.scan(advance, initial, (states, jnp.exp(block_totals)))
    carried = jnp.einsum('clgn,cgrpn,cgrl->clgrp', query_blocks, entering, jnp.exp(cumulative), precision=precise)
    return ((within + carried).reshape(length, groups, per_group, width), final)

def one_group(members):
    value_part, step_part, log_part, key_part, query_part = members
    result = blockwise(value_part[:, None], step_part[None], log_part[None], key_part, query_part)[0]
    return result[:, 0]

def normalize(rows, gain):
    widened = rows.astype(jnp.float32)
    scaled = widened * lax.rsqrt(lax.optimization_barrier(jnp.mean(widened * widened, axis=-1, keepdims=True)) + epsilon)
    return (scaled * gain).astype(jnp.bfloat16)

def reference(skip_stream_entering, content_signal_matrix, writer_signal_matrix, reader_signal_matrix, multiplier_signal, interval_before_softplus, extra_log_shrink, log_forget_speed, content_filter_coefs, writer_filter_coefs, reader_filter_coefs, skip_path_factor, cluster_scaling_vector, blend_result_matrix, feature_blend_scaling, widening_matrix, narrowing_matrix):
    per_group = HEADS // GROUPS
    values = convolve(content_signal_matrix, content_filter_coefs)
    key_rows = convolve(writer_signal_matrix, writer_filter_coefs)
    query_rows = convolve(reader_signal_matrix, reader_filter_coefs)
    interval_lengths = jax.nn.softplus(interval_before_softplus)
    log_forgetting = extra_log_shrink - jnp.exp(log_forget_speed)[:, None] * interval_lengths
    members = (jnp.transpose(values.reshape(TOKENS, GROUPS, per_group, HEAD_DIM), (1, 0, 2, 3)), interval_lengths.reshape(GROUPS, per_group, TOKENS), log_forgetting.reshape(GROUPS, per_group, TOKENS), jnp.transpose(key_rows.reshape(TOKENS, GROUPS, STATE), (1, 0, 2)), jnp.transpose(query_rows.reshape(TOKENS, GROUPS, STATE), (1, 0, 2)))
    scan_out = jnp.transpose(lax.map(one_group, members), (1, 0, 2, 3)).reshape(TOKENS, D_INNER)
    gated = (scan_out + jnp.repeat(skip_path_factor, HEAD_DIM) * values) * jax.nn.silu(multiplier_signal.astype(jnp.float32))
    grouped = gated.reshape(TOKENS, GROUPS, D_INNER // GROUPS)
    grouped = grouped * lax.rsqrt(lax.optimization_barrier(jnp.mean(grouped * grouped, axis=-1, keepdims=True)) + epsilon)
    heads_out = (grouped.reshape(TOKENS, D_INNER) * cluster_scaling_vector).astype(jnp.bfloat16)
    part_width = D_INNER // N_TP
    mixer_sum = jnp.zeros((TOKENS, D), jnp.float32)
    for index in range(N_TP):
        partial_term = jnp.dot(heads_out[:, index * part_width:(index + 1) * part_width], blend_result_matrix[index * part_width:(index + 1) * part_width], preferred_element_type=jnp.float32)
        mixer_sum = mixer_sum + lax.optimization_barrier(partial_term.astype(jnp.bfloat16)).astype(jnp.float32)
    mixer_out = mixer_sum.astype(jnp.bfloat16)
    layer_state = (skip_stream_entering.astype(jnp.float32) + mixer_out.astype(jnp.float32)).astype(jnp.bfloat16)
    normed = normalize(layer_state, feature_blend_scaling)
    hidden_width = FF // N_TP
    mlp_sum = jnp.zeros((TOKENS, D), jnp.float32)
    for index in range(N_TP):
        lifted = jax.nn.relu(jnp.dot(normed, widening_matrix[:, index * hidden_width:(index + 1) * hidden_width], preferred_element_type=jnp.float32))
        hidden = (lifted * lifted).astype(jnp.bfloat16)
        partial_term = jnp.dot(hidden, narrowing_matrix[index * hidden_width:(index + 1) * hidden_width], preferred_element_type=jnp.float32)
        mlp_sum = mlp_sum + lax.optimization_barrier(partial_term.astype(jnp.bfloat16)).astype(jnp.float32)
    mlp_out = mlp_sum.astype(jnp.bfloat16)
    return (layer_state.astype(jnp.float32) + mlp_out.astype(jnp.float32)).astype(jnp.bfloat16)
```

```python
import jax
import jax.numpy as jnp
from jax import lax
from jax.experimental import pallas as pl
from jax.experimental.pallas import tpu as pltpu
from jax.sharding import Mesh
from jax.sharding import PartitionSpec as P

HEADS = 8
HEAD_DIM = 64
STATE = 128
BLOCK = 128
WIDTH = HEADS * HEAD_DIM
RIM = 8
SP = ("z", "y")
TP = ("x", "c")
ROWS = ("y", "x")
EPSILON = 1e-05
INTERPRET = False

f32 = jnp.float32
bf16 = jnp.bfloat16
VMEM = pl.BlockSpec(memory_space=pltpu.VMEM)
SMEM = pl.BlockSpec(memory_space=pltpu.SMEM)
HBM = pl.BlockSpec(memory_space=pl.ANY)


def call(kernel, outs, in_specs, scratch=(), **kw):
    single = not isinstance(outs, (list, tuple))
    return pl.pallas_call(
        kernel,
        out_shape=outs,
        in_specs=in_specs,
        out_specs=VMEM if single else [VMEM] * len(outs),
        scratch_shapes=list(scratch),
        interpret=INTERPRET,
        **kw,
    )


def shape(dims, kind):
    return jax.ShapeDtypeStruct(dims, kind)


def exchange(value, axes):
    return lax.all_to_all(value, axes, split_axis=0, concat_axis=0, tiled=True)


def dot(a, b, dims, **kw):
    return lax.dot_general(a, b, (dims, ((), ())), preferred_element_type=f32, **kw)


def spread(rows, width):
    head = lax.broadcasted_iota(jnp.int32, (HEADS, HEADS * width), 0)
    lane = lax.broadcasted_iota(jnp.int32, (HEADS, HEADS * width), 1)
    chosen = jnp.where(lane // width == head, 1.0, 0.0).astype(f32)
    return dot(rows, chosen, ((0,), (0,)), precision=lax.Precision.HIGHEST)


def silu(value):
    return value / (1.0 + jnp.exp(-value))


def convolve(src_ref, rim, taps_ref, room):
    room[0:RIM, :] = rim.astype(f32)
    room[RIM : RIM + BLOCK, :] = src_ref[...].astype(f32)
    taps = taps_ref[...].astype(f32)
    width = taps.shape[0]
    total = None
    for k in range(width):
        start = RIM - width + 1 + k
        term = room[start : start + BLOCK, :] * taps[k : k + 1, :]
        total = term if total is None else total + term
    return silu(total)


def local_kernel(
    x_ref, b_ref, c_ref, rim_ref, xt_ref, bt_ref, ct_ref, dt_ref, shrink_ref, speed_ref, skip_ref,
    pre_ref, query_ref, cum_ref, send_ref, x_room, b_room, c_room,
):
    values = convolve(x_ref, rim_ref[:, 0:WIDTH], xt_ref, x_room)
    keys = convolve(b_ref, rim_ref[:, WIDTH : WIDTH + STATE], bt_ref, b_room).astype(bf16)
    query = convolve(c_ref, rim_ref[:, WIDTH + STATE : WIDTH + 2 * STATE], ct_ref, c_room).astype(bf16)
    query_ref[...] = query
    before = dt_ref[...]
    steps = jnp.maximum(before, 0.0) + jnp.log1p(jnp.exp(-jnp.abs(before)))
    head = lax.broadcasted_iota(jnp.int32, (HEADS, BLOCK), 0)
    token = lax.broadcasted_iota(jnp.int32, (HEADS, BLOCK), 1)
    speed = jnp.zeros((HEADS, BLOCK), f32)
    for h in range(HEADS):
        speed = jnp.where(head == h, speed_ref[h], speed)
    cum = shrink_ref[...] - jnp.exp(speed) * steps
    reach = 1
    while reach < BLOCK:
        cum = cum + jnp.where(token >= reach, pltpu.roll(cum, reach, 1), 0.0)
        reach *= 2
    cum_ref[...] = cum
    last = cum[:, BLOCK - 1 : BLOCK]
    weight = steps * jnp.exp(last - cum)
    weighted = (values * spread(weight, HEAD_DIM)).astype(bf16)
    state = dot(weighted, keys, ((0,), (0,)))
    send_ref[:, 0:8, :] = state.reshape(WIDTH // 8, 8, STATE).astype(bf16)
    row = lax.broadcasted_iota(jnp.int32, (8, STATE), 0)
    for h in range(HEADS):
        whole = jnp.broadcast_to(last[h : h + 1, :], (8, STATE))
        high = whole.astype(bf16).astype(f32)
        both = jnp.where(row == 0, high, jnp.where(row == 1, whole - high, 0.0)).astype(bf16)
        for k in range(HEAD_DIM // 8):
            send_ref[h * (HEAD_DIM // 8) + k, 8:16, :] = both
    scores = dot(query, keys, ((1,), (1,)))
    columns = spread(cum, BLOCK)
    later = lax.broadcasted_iota(jnp.int32, (BLOCK, BLOCK), 0)
    earlier = lax.broadcasted_iota(jnp.int32, (BLOCK, BLOCK), 1)
    causal = later >= earlier
    first = lax.broadcasted_iota(jnp.int32, (BLOCK, 2 * HEAD_DIM), 1) < HEAD_DIM
    for pair in range(HEADS // 2):
        lanes = slice(pair * 2 * HEAD_DIM, (pair + 1) * 2 * HEAD_DIM)
        two = values[:, lanes]
        two_low = two.astype(bf16)
        parts = []
        for h in (2 * pair, 2 * pair + 1):
            away = columns[:, h * BLOCK : (h + 1) * BLOCK] - cum[h : h + 1, :]
            mixing = scores * jnp.exp(jnp.where(causal, away, -jnp.inf)) * steps[h : h + 1, :]
            parts.append(dot(mixing.astype(bf16), two_low, ((1,), (0,))))
        within = jnp.where(first, parts[0], parts[1])
        skip = jnp.where(first, skip_ref[2 * pair], skip_ref[2 * pair + 1])
        pre_ref[:, lanes] = within + skip * two


def scan_kernel(got_ref, out_ref):
    carried = jnp.zeros((8, STATE), f32)
    for k in range(got_ref.shape[0]):
        out_ref[k] = carried.astype(bf16)
        tile = got_ref[k].astype(f32)
        factor = jnp.exp(tile[8:9, :] + tile[9:10, :])
        carried = carried * factor + tile[0:8, :]


def gate_kernel(pre_ref, query_ref, cum_ref, inc_ref, gate_ref, gain_ref, w_ref, out_ref):
    inc = inc_ref[...].reshape(WIDTH, STATE)
    arriving = dot(query_ref[...], inc, ((1,), (1,))) * spread(jnp.exp(cum_ref[...]), HEAD_DIM)
    gated = (pre_ref[...] + arriving) * silu(gate_ref[...].astype(f32))
    scale = lax.rsqrt(jnp.mean(gated * gated, axis=-1, keepdims=True) + EPSILON)
    heads_out = (gated * scale * gain_ref[...]).astype(bf16)
    out = dot(heads_out, w_ref[...], ((1,), (0,))).astype(bf16)
    out_ref[...] = out.reshape(out_ref.shape)


def norm_kernel(got_ref, skip_ref, gain_ref, own_ref, copies_ref):
    total = got_ref[0].astype(f32)
    for k in range(1, got_ref.shape[0]):
        total = total + got_ref[k].astype(f32)
    own = (skip_ref[...].astype(f32) + total.astype(bf16).astype(f32)).astype(bf16)
    own_ref[...] = own
    wide = own.astype(f32)
    scale = lax.rsqrt(jnp.mean(wide * wide, axis=-1, keepdims=True) + EPSILON)
    normed = (wide * scale * gain_ref[...]).astype(bf16)
    for k in range(copies_ref.shape[0]):
        copies_ref[k] = normed


def mlp_kernel(rows_ref, w_ref, out_ref, w_vmem, sems):
    halves, depth, both = w_ref.shape
    units = both // 2
    pieces = sems.shape[1]
    size = depth // pieces
    copies = []
    for j in range(pieces):
        for k in range(halves):
            copy = pltpu.make_async_copy(
                w_ref.at[k, pl.ds(j * size, size)], w_vmem.at[k, pl.ds(j * size, size)], sems.at[k, j]
            )
            copy.start()
            copies.append(copy)
    count, each, _ = rows_ref.shape
    rows = rows_ref[...].reshape(count * each, depth)
    lifted = [None] * halves
    for j in range(pieces):
        for k in range(halves):
            copies[j * halves + k].wait()
            part = dot(rows[:, j * size : (j + 1) * size], w_vmem[k, j * size : (j + 1) * size, 0:units], ((1,), (0,)))
            lifted[k] = part if lifted[k] is None else lifted[k] + part
    hidden = []
    for k in range(halves):
        up = jnp.maximum(lifted[k], 0.0)
        hidden.append((up * up).astype(bf16))
    for j in range(pieces):
        total = None
        for k in range(halves):
            part = dot(hidden[k], w_vmem[k, j * size : (j + 1) * size, units:both], ((1,), (1,)))
            total = part if total is None else total + part
        out_ref[:, :, j * size : (j + 1) * size] = total.astype(bf16).reshape(count, each, size)


def final_kernel(got_ref, own_ref, out_ref):
    total = got_ref[0].astype(f32)
    for k in range(1, got_ref.shape[0]):
        total = total + got_ref[k].astype(f32)
    out_ref[...] = (own_ref[...].astype(f32) + total.astype(bf16).astype(f32)).astype(bf16)


def per_device(
    skip_stream_entering,
    content_signal_matrix,
    writer_signal_matrix,
    reader_signal_matrix,
    multiplier_signal,
    interval_before_softplus,
    extra_log_shrink,
    log_forget_speed,
    content_filter_coefs,
    writer_filter_coefs,
    reader_filter_coefs,
    skip_path_factor,
    cluster_scaling_vector,
    blend_result_matrix,
    feature_blend_scaling,
    widening_matrix,
    narrowing_matrix,
):
    ny = lax.axis_size("y")
    nsp = lax.axis_size("z") * ny
    ntp = lax.axis_size("x") * lax.axis_size("c")
    nrows = ny * lax.axis_size("x")
    width = skip_stream_entering.shape[1]
    own_count = skip_stream_entering.shape[0]

    rim = jnp.concatenate(
        [
            content_signal_matrix[BLOCK - RIM :],
            writer_signal_matrix[BLOCK - RIM :],
            reader_signal_matrix[BLOCK - RIM :],
        ],
        axis=1,
    )
    rim = lax.ppermute(rim, SP, [(k, k + 1) for k in range(nsp - 1)])

    depth, units = widening_matrix.shape
    slim = units // ny
    mine = jnp.concatenate(
        [widening_matrix.reshape(depth, ny, slim), narrowing_matrix.T.reshape(depth, ny, slim)], axis=2
    )
    mine = jnp.moveaxis(mine, 1, 0)
    parts = exchange(mine, "y").reshape(ny * depth, 2 * slim)
    weights = lax.all_gather(parts, ("c", "z"), axis=0, tiled=True).reshape(-1, width, 2 * slim)

    rim, content_signal_matrix, parts = lax.optimization_barrier((rim, content_signal_matrix, parts))
    pre, query, cum, send = call(
        local_kernel,
        [
            shape((BLOCK, WIDTH), f32),
            shape((BLOCK, STATE), bf16),
            shape((HEADS, BLOCK), f32),
            shape((nsp, 16, STATE), bf16),
        ],
        [VMEM] * 9 + [SMEM] * 2,
        [pltpu.VMEM((RIM + BLOCK, n), f32) for n in (WIDTH, STATE, STATE)],
    )(
        content_signal_matrix,
        writer_signal_matrix,
        reader_signal_matrix,
        rim,
        content_filter_coefs,
        writer_filter_coefs,
        reader_filter_coefs,
        interval_before_softplus,
        extra_log_shrink,
        log_forget_speed,
        skip_path_factor,
    )
    got = exchange(send, SP)
    before = call(scan_kernel, shape((nsp, 8, STATE), bf16), [VMEM])(got)
    incoming = exchange(before, SP)
    mixed = call(gate_kernel, shape((ntp, own_count, width), bf16), [VMEM] * 7)(
        pre,
        query,
        cum,
        incoming,
        multiplier_signal,
        cluster_scaling_vector.reshape(1, -1),
        blend_result_matrix,
    )
    mixed = exchange(mixed, TP)
    own, copies = call(
        norm_kernel,
        [shape((own_count, width), bf16), shape((nrows, own_count, width), bf16)],
        [VMEM] * 3,
    )(mixed, skip_stream_entering, feature_blend_scaling.reshape(1, -1))
    rows = exchange(copies, ROWS)
    out = call(
        mlp_kernel,
        shape((nrows, own_count, width), bf16),
        [VMEM, HBM],
        [pltpu.VMEM(weights.shape, bf16), pltpu.SemaphoreType.DMA((weights.shape[0], 4))],
    )(rows, weights)
    out = exchange(out, ROWS)
    return call(final_kernel, shape((own_count, width), bf16), [VMEM] * 2)(out, own)


def solution(mesh):
    torus = Mesh(mesh.devices.reshape(16, 4, 4, 2), ("z", "y", "x", "c"))
    placed = (
        P(SP + TP, None),
        P(SP, TP),
        P(SP, TP),
        P(SP, TP),
        P(SP, TP),
        P(TP, SP),
        P(TP, SP),
        P(TP),
        P(None, TP),
        P(None, TP),
        P(None, TP),
        P(TP),
        P(TP),
        P(TP, None),
        P(),
        P(SP, TP),
        P(TP, SP),
    )
    return jax.shard_map(
        per_device, mesh=torus, in_specs=placed, out_specs=P(SP + TP, None), check_vma=False
    )
```

```python
import jax
import jax.numpy as jnp
from jax import lax
from jax.experimental import pallas as pl
from jax.experimental.pallas import tpu as pltpu
from jax.sharding import Mesh
from jax.sharding import PartitionSpec as P

HEADS = 8
HEAD_DIM = 64
STATE = 128
BLOCK = 128
WIDTH = HEADS * HEAD_DIM
RIM = 8
SP = ("z", "y")
TP = ("x", "c")
ROWS = ("y", "x")
EPSILON = 1e-05
INTERPRET = False

f32 = jnp.float32
bf16 = jnp.bfloat16
VMEM = pl.BlockSpec(memory_space=pltpu.VMEM)
SMEM = pl.BlockSpec(memory_space=pltpu.SMEM)
HBM = pl.BlockSpec(memory_space=pl.ANY)


def call(kernel, outs, in_specs, scratch=(), **kw):
    single = not isinstance(outs, (list, tuple))
    return pl.pallas_call(
        kernel,
        out_shape=outs,
        in_specs=in_specs,
        out_specs=VMEM if single else [VMEM] * len(outs),
        scratch_shapes=list(scratch),
        interpret=INTERPRET,
        **kw,
    )


def shape(dims, kind):
    return jax.ShapeDtypeStruct(dims, kind) if INTERPRET else pltpu.VMEM(dims, kind)


def near(value):
    return value if INTERPRET else pltpu.with_memory_space_constraint(value, pltpu.VMEM)


def exchange(value, axes):
    return lax.all_to_all(value, axes, split_axis=0, concat_axis=0, tiled=True)


def dot(a, b, dims, **kw):
    return lax.dot_general(a, b, (dims, ((), ())), preferred_element_type=f32, **kw)


def spread(rows, width):
    head = lax.broadcasted_iota(jnp.int32, (HEADS, HEADS * width), 0)
    lane = lax.broadcasted_iota(jnp.int32, (HEADS, HEADS * width), 1)
    chosen = jnp.where(lane // width == head, 1.0, 0.0).astype(f32)
    return dot(rows, chosen, ((0,), (0,)), precision=lax.Precision.HIGHEST)


def silu(value):
    return value / (1.0 + jnp.exp(-value))


def convolve(src_ref, rim, taps_ref, room):
    room[0:RIM, :] = rim.astype(f32)
    room[RIM : RIM + BLOCK, :] = src_ref[...].astype(f32)
    taps = taps_ref[...].astype(f32)
    width = taps.shape[0]
    total = None
    for k in range(width):
        start = RIM - width + 1 + k
        term = room[start : start + BLOCK, :] * taps[k : k + 1, :]
        total = term if total is None else total + term
    return silu(total)


def first_kernel(x_ref, b_ref, c_ref, up_ref, down_ref, rim_ref, mine_ref):
    rim_ref[:, 0:WIDTH] = x_ref[...]
    rim_ref[:, WIDTH : WIDTH + STATE] = b_ref[...]
    rim_ref[:, WIDTH + STATE : WIDTH + 2 * STATE] = c_ref[...]
    slim = mine_ref.shape[2] // 2
    for k in range(mine_ref.shape[0]):
        mine_ref[k, :, 0:slim] = up_ref[:, k * slim : (k + 1) * slim]
        mine_ref[k, :, slim : 2 * slim] = down_ref[:, k * slim : (k + 1) * slim]


def local_kernel(
    x_ref, b_ref, c_ref, rim_ref, xt_ref, bt_ref, ct_ref, dt_ref, shrink_ref, speed_ref, skip_ref,
    pre_ref, query_ref, cum_ref, send_ref, x_room, b_room, c_room,
):
    values = convolve(x_ref, rim_ref[:, 0:WIDTH], xt_ref, x_room)
    keys = convolve(b_ref, rim_ref[:, WIDTH : WIDTH + STATE], bt_ref, b_room).astype(bf16)
    query = convolve(c_ref, rim_ref[:, WIDTH + STATE : WIDTH + 2 * STATE], ct_ref, c_room).astype(bf16)
    query_ref[...] = query
    before = dt_ref[...]
    steps = jnp.maximum(before, 0.0) + jnp.log1p(jnp.exp(-jnp.abs(before)))
    head = lax.broadcasted_iota(jnp.int32, (HEADS, BLOCK), 0)
    token = lax.broadcasted_iota(jnp.int32, (HEADS, BLOCK), 1)
    speed = jnp.zeros((HEADS, BLOCK), f32)
    for h in range(HEADS):
        speed = jnp.where(head == h, speed_ref[h], speed)
    cum = shrink_ref[...] - jnp.exp(speed) * steps
    reach = 1
    while reach < BLOCK:
        cum = cum + jnp.where(token >= reach, pltpu.roll(cum, reach, 1), 0.0)
        reach *= 2
    cum_ref[...] = cum
    last = cum[:, BLOCK - 1 : BLOCK]
    weight = steps * jnp.exp(last - cum)
    weighted = (values * spread(weight, HEAD_DIM)).astype(bf16)
    state = dot(weighted, keys, ((0,), (0,)))
    send_ref[:, 0:8, :] = state.reshape(WIDTH // 8, 8, STATE).astype(bf16)
    row = lax.broadcasted_iota(jnp.int32, (8, STATE), 0)
    for h in range(HEADS):
        whole = jnp.broadcast_to(last[h : h + 1, :], (8, STATE))
        high = whole.astype(bf16).astype(f32)
        both = jnp.where(row == 0, high, jnp.where(row == 1, whole - high, 0.0)).astype(bf16)
        for k in range(HEAD_DIM // 8):
            send_ref[h * (HEAD_DIM // 8) + k, 8:16, :] = both
    scores = dot(query, keys, ((1,), (1,)))
    columns = spread(cum, BLOCK)
    later = lax.broadcasted_iota(jnp.int32, (BLOCK, BLOCK), 0)
    earlier = lax.broadcasted_iota(jnp.int32, (BLOCK, BLOCK), 1)
    causal = later >= earlier
    first = lax.broadcasted_iota(jnp.int32, (BLOCK, 2 * HEAD_DIM), 1) < HEAD_DIM
    for pair in range(HEADS // 2):
        lanes = slice(pair * 2 * HEAD_DIM, (pair + 1) * 2 * HEAD_DIM)
        two = values[:, lanes]
        two_low = two.astype(bf16)
        parts = []
        for h in (2 * pair, 2 * pair + 1):
            away = columns[:, h * BLOCK : (h + 1) * BLOCK] - cum[h : h + 1, :]
            mixing = scores * jnp.exp(jnp.where(causal, away, -jnp.inf)) * steps[h : h + 1, :]
            parts.append(dot(mixing.astype(bf16), two_low, ((1,), (0,))))
        within = jnp.where(first, parts[0], parts[1])
        skip = jnp.where(first, skip_ref[2 * pair], skip_ref[2 * pair + 1])
        pre_ref[:, lanes] = within + skip * two


def scan_kernel(got_ref, out_ref):
    carried = jnp.zeros((8, STATE), f32)
    for k in range(got_ref.shape[0]):
        out_ref[k] = carried.astype(bf16)
        tile = got_ref[k].astype(f32)
        factor = jnp.exp(tile[8:9, :] + tile[9:10, :])
        carried = carried * factor + tile[0:8, :]


def gate_kernel(pre_ref, query_ref, cum_ref, inc_ref, gate_ref, gain_ref, w_ref, out_ref, w_room, sem):
    copy = pltpu.make_async_copy(w_ref, w_room, sem)
    copy.start()
    inc = inc_ref[...].reshape(WIDTH, STATE)
    arriving = dot(query_ref[...], inc, ((1,), (1,))) * spread(jnp.exp(cum_ref[...]), HEAD_DIM)
    gated = (pre_ref[...] + arriving) * silu(gate_ref[...].astype(f32))
    scale = lax.rsqrt(jnp.mean(gated * gated, axis=-1, keepdims=True) + EPSILON)
    heads_out = (gated * scale * gain_ref[...]).astype(bf16)
    copy.wait()
    out = dot(heads_out, w_room[...], ((1,), (0,))).astype(bf16)
    out_ref[...] = out.reshape(out_ref.shape)


def norm_kernel(got_ref, skip_ref, gain_ref, own_ref, copies_ref):
    total = got_ref[0].astype(f32)
    for k in range(1, got_ref.shape[0]):
        total = total + got_ref[k].astype(f32)
    own = (skip_ref[...].astype(f32) + total.astype(bf16).astype(f32)).astype(bf16)
    own_ref[...] = own
    wide = own.astype(f32)
    scale = lax.rsqrt(jnp.mean(wide * wide, axis=-1, keepdims=True) + EPSILON)
    normed = (wide * scale * gain_ref[...]).astype(bf16)
    for k in range(copies_ref.shape[0]):
        copies_ref[k] = normed


def mlp_kernel(rows_ref, w_ref, out_ref, w_vmem, sems):
    halves, depth, both = w_ref.shape
    units = both // 2
    pieces = sems.shape[1]
    size = depth // pieces
    copies = []
    for j in range(pieces):
        for k in range(halves):
            copy = pltpu.make_async_copy(
                w_ref.at[k, pl.ds(j * size, size)], w_vmem.at[k, pl.ds(j * size, size)], sems.at[k, j]
            )
            copy.start()
            copies.append(copy)
    count, each, _ = rows_ref.shape
    rows = rows_ref[...].reshape(count * each, depth)
    lifted = [None] * halves
    for j in range(pieces):
        for k in range(halves):
            copies[j * halves + k].wait()
            part = dot(rows[:, j * size : (j + 1) * size], w_vmem[k, j * size : (j + 1) * size, 0:units], ((1,), (0,)))
            lifted[k] = part if lifted[k] is None else lifted[k] + part
    hidden = []
    for k in range(halves):
        up = jnp.maximum(lifted[k], 0.0)
        hidden.append((up * up).astype(bf16))
    for j in range(pieces):
        total = None
        for k in range(halves):
            part = dot(hidden[k], w_vmem[k, j * size : (j + 1) * size, units:both], ((1,), (1,)))
            total = part if total is None else total + part
        out_ref[:, :, j * size : (j + 1) * size] = total.astype(bf16).reshape(count, each, size)


def final_kernel(got_ref, own_ref, out_ref):
    total = got_ref[0].astype(f32)
    for k in range(1, got_ref.shape[0]):
        total = total + got_ref[k].astype(f32)
    out_ref[...] = (own_ref[...].astype(f32) + total.astype(bf16).astype(f32)).astype(bf16)


def per_device(
    skip_stream_entering,
    content_signal_matrix,
    writer_signal_matrix,
    reader_signal_matrix,
    multiplier_signal,
    interval_before_softplus,
    extra_log_shrink,
    log_forget_speed,
    content_filter_coefs,
    writer_filter_coefs,
    reader_filter_coefs,
    skip_path_factor,
    cluster_scaling_vector,
    blend_result_matrix,
    feature_blend_scaling,
    widening_matrix,
    narrowing_matrix,
):
    ny = lax.axis_size("y")
    nsp = lax.axis_size("z") * ny
    ntp = lax.axis_size("x") * lax.axis_size("c")
    nrows = ny * lax.axis_size("x")
    width = skip_stream_entering.shape[1]
    own_count = skip_stream_entering.shape[0]

    depth, units = widening_matrix.shape
    slim = units // ny
    rim, mine = pl.pallas_call(
        first_kernel,
        grid=(1,),
        out_shape=[shape((RIM, WIDTH + 2 * STATE), bf16), shape((ny, depth, 2 * slim), bf16)],
        in_specs=[pl.BlockSpec((RIM, n), lambda i: (BLOCK // RIM - 1, 0)) for n in (WIDTH, STATE, STATE)]
        + [pl.BlockSpec((depth, units), lambda i: (0, 0))] * 2,
        out_specs=[
            pl.BlockSpec((RIM, WIDTH + 2 * STATE), lambda i: (0, 0)),
            pl.BlockSpec((ny, depth, 2 * slim), lambda i: (0, 0, 0)),
        ],
        interpret=INTERPRET,
    )(content_signal_matrix, writer_signal_matrix, reader_signal_matrix, widening_matrix, narrowing_matrix.T)
    rim = lax.ppermute(rim, SP, [(k, k + 1) for k in range(nsp - 1)])
    parts = exchange(mine, "y").reshape(ny * depth, 2 * slim)
    weights = lax.all_gather(parts, ("c", "z"), axis=0, tiled=True).reshape(-1, width, 2 * slim)

    rim, parts = lax.optimization_barrier((rim, parts))
    pre, query, cum, send = call(
        local_kernel,
        [
            shape((BLOCK, WIDTH), f32),
            shape((BLOCK, STATE), bf16),
            shape((HEADS, BLOCK), f32),
            shape((nsp, 16, STATE), bf16),
        ],
        [VMEM] * 9 + [SMEM] * 2,
        [pltpu.VMEM((RIM + BLOCK, n), f32) for n in (WIDTH, STATE, STATE)],
    )(
        content_signal_matrix,
        writer_signal_matrix,
        reader_signal_matrix,
        near(rim),
        content_filter_coefs,
        writer_filter_coefs,
        reader_filter_coefs,
        interval_before_softplus,
        extra_log_shrink,
        log_forget_speed,
        skip_path_factor,
    )
    got = exchange(send, SP)
    before = call(scan_kernel, shape((nsp, 8, STATE), bf16), [VMEM])(near(got))
    incoming = exchange(before, SP)
    mixed = call(
        gate_kernel,
        shape((ntp, own_count, width), bf16),
        [VMEM] * 6 + [HBM],
        [pltpu.VMEM(blend_result_matrix.shape, bf16), pltpu.SemaphoreType.DMA(())],
    )(
        near(pre),
        near(query),
        near(cum),
        near(incoming),
        multiplier_signal,
        cluster_scaling_vector.reshape(1, -1),
        blend_result_matrix,
    )
    mixed = exchange(mixed, TP)
    own, copies = call(
        norm_kernel,
        [shape((own_count, width), bf16), shape((nrows, own_count, width), bf16)],
        [VMEM] * 3,
    )(near(mixed), skip_stream_entering, feature_blend_scaling.reshape(1, -1))
    rows = exchange(copies, ROWS)
    out = call(
        mlp_kernel,
        shape((nrows, own_count, width), bf16),
        [VMEM, HBM],
        [pltpu.VMEM(weights.shape, bf16), pltpu.SemaphoreType.DMA((weights.shape[0], 4))],
    )(near(rows), weights)
    out = exchange(out, ROWS)
    return call(final_kernel, jax.ShapeDtypeStruct((own_count, width), bf16), [VMEM] * 2)(near(out), near(own))


def solution(mesh):
    torus = Mesh(mesh.devices.reshape(16, 4, 4, 2), ("z", "y", "x", "c"))
    placed = (
        P(SP + TP, None),
        P(SP, TP),
        P(SP, TP),
        P(SP, TP),
        P(SP, TP),
        P(TP, SP),
        P(TP, SP),
        P(TP),
        P(None, TP),
        P(None, TP),
        P(None, TP),
        P(TP),
        P(TP),
        P(TP, None),
        P(),
        P(SP, TP),
        P(TP, SP),
    )
    return jax.shard_map(
        per_device, mesh=torus, in_specs=placed, out_specs=P(SP + TP, None), check_vma=False
    )
```

```python
import jax
import jax.numpy as jnp
from jax import lax
from jax.experimental import pallas as pl
from jax.experimental.pallas import tpu as pltpu
from jax.sharding import Mesh
from jax.sharding import PartitionSpec as P

HEADS = 8
HEAD_DIM = 64
STATE = 128
BLOCK = 128
WIDTH = HEADS * HEAD_DIM
RIM = 8
PAIR = 2 * HEAD_DIM
TAIL = 16
SP = ("zh", "zl", "y")
TP = ("x", "c")
ROWS = ("y", "x")
EPSILON = 1e-05
INTERPRET = False

f32 = jnp.float32
bf16 = jnp.bfloat16
VMEM = pl.BlockSpec(memory_space=pltpu.VMEM)
SMEM = pl.BlockSpec(memory_space=pltpu.SMEM)
HBM = pl.BlockSpec(memory_space=pl.ANY)


def call(kernel, outs, in_specs, scratch=(), **kw):
    single = not isinstance(outs, (list, tuple))
    return pl.pallas_call(
        kernel,
        out_shape=outs,
        in_specs=in_specs,
        out_specs=VMEM if single else [VMEM] * len(outs),
        scratch_shapes=list(scratch),
        interpret=INTERPRET,
        **kw,
    )


def shape(dims, kind):
    return jax.ShapeDtypeStruct(dims, kind) if INTERPRET else pltpu.VMEM(dims, kind)


def near(value):
    return value if INTERPRET else pltpu.with_memory_space_constraint(value, pltpu.VMEM)


def exchange(value, axes):
    return lax.all_to_all(value, axes, split_axis=0, concat_axis=0, tiled=True)


def dot(a, b, dims, **kw):
    return lax.dot_general(a, b, (dims, ((), ())), preferred_element_type=f32, **kw)


def spread(rows, width):
    head = lax.broadcasted_iota(jnp.int32, (HEADS, HEADS * width), 0)
    lane = lax.broadcasted_iota(jnp.int32, (HEADS, HEADS * width), 1)
    chosen = jnp.where(lane // width == head, 1.0, 0.0).astype(f32)
    return dot(rows, chosen, ((0,), (0,)), precision=lax.Precision.HIGHEST)


def silu(value):
    return value / (1.0 + jnp.exp(-value))


def convolve(src_ref, rim, taps_ref, room):
    room[0:RIM, :] = rim.astype(f32)
    room[RIM : RIM + BLOCK, :] = src_ref[...].astype(f32)
    taps = taps_ref[...].astype(f32)
    width = taps.shape[0]
    total = None
    for k in range(width):
        start = RIM - width + 1 + k
        term = room[start : start + BLOCK, :] * taps[k : k + 1, :]
        total = term if total is None else total + term
    return silu(total)


def put_state(ref, place, start, state, logs):
    ref[place, start : start + PAIR, :] = state.astype(bf16)
    row = lax.broadcasted_iota(jnp.int32, (TAIL, STATE), 0)
    tail = jnp.zeros((TAIL, STATE), f32)
    for h in range(2):
        whole = jnp.broadcast_to(logs[h : h + 1, :], (TAIL, STATE))
        high = whole.astype(bf16).astype(f32)
        tail = jnp.where(row == 2 * h, high, jnp.where(row == 2 * h + 1, whole - high, tail))
    ref[place, start + PAIR : start + PAIR + TAIL, :] = tail.astype(bf16)


def take_state(ref, place, start):
    state = ref[place, start : start + PAIR, :].astype(f32)
    tail = ref[place, start + PAIR : start + PAIR + TAIL, :].astype(f32)
    return state, jnp.concatenate([tail[2 * h : 2 * h + 1, :] + tail[2 * h + 1 : 2 * h + 2, :] for h in range(2)], axis=0)


def factor(logs):
    grown = jnp.exp(logs)
    return jnp.concatenate([jnp.broadcast_to(grown[h : h + 1, :], (HEAD_DIM, STATE)) for h in range(2)], axis=0)


def first_kernel(x_ref, b_ref, c_ref, rim_ref):
    rim_ref[:, 0:WIDTH] = x_ref[...]
    rim_ref[:, WIDTH : WIDTH + STATE] = b_ref[...]
    rim_ref[:, WIDTH + STATE : WIDTH + 2 * STATE] = c_ref[...]


def local_kernel(
    x_ref, b_ref, c_ref, rim_ref, xt_ref, bt_ref, ct_ref, dt_ref, shrink_ref, up_ref, down_ref, speed_ref, skip_ref,
    pre_ref, query_ref, cum_ref, send_ref, x_room, b_room, c_room,
):
    values = convolve(x_ref, rim_ref[:, 0:WIDTH], xt_ref, x_room)
    keys = convolve(b_ref, rim_ref[:, WIDTH : WIDTH + STATE], bt_ref, b_room).astype(bf16)
    query = convolve(c_ref, rim_ref[:, WIDTH + STATE : WIDTH + 2 * STATE], ct_ref, c_room).astype(bf16)
    query_ref[...] = query
    before = dt_ref[...]
    steps = jnp.maximum(before, 0.0) + jnp.log1p(jnp.exp(-jnp.abs(before)))
    head = lax.broadcasted_iota(jnp.int32, (HEADS, BLOCK), 0)
    token = lax.broadcasted_iota(jnp.int32, (HEADS, BLOCK), 1)
    speed = jnp.zeros((HEADS, BLOCK), f32)
    for h in range(HEADS):
        speed = jnp.where(head == h, speed_ref[h], speed)
    cum = shrink_ref[...] - jnp.exp(speed) * steps
    reach = 1
    while reach < BLOCK:
        cum = cum + jnp.where(token >= reach, pltpu.roll(cum, reach, 1), 0.0)
        reach *= 2
    cum_ref[...] = cum
    last = cum[:, BLOCK - 1 : BLOCK]
    weight = steps * jnp.exp(last - cum)
    weighted = (values * spread(weight, HEAD_DIM)).astype(bf16)
    state = dot(weighted, keys, ((0,), (0,)))
    pieces = send_ref.shape[0]
    depth, units = up_ref.shape
    slabs = units // pieces // STATE
    for k in range(pieces):
        for j in range(slabs):
            lanes = slice((k * slabs + j) * STATE, (k * slabs + j + 1) * STATE)
            send_ref[k, j * depth : (j + 1) * depth, :] = up_ref[:, lanes]
            send_ref[k, (slabs + j) * depth : (slabs + j + 1) * depth, :] = down_ref[:, lanes]
        put_state(send_ref, k, 2 * slabs * depth, state[k * PAIR : (k + 1) * PAIR, :], last[2 * k : 2 * k + 2, :])
    scores = dot(query, keys, ((1,), (1,)))
    columns = spread(cum, BLOCK)
    later = lax.broadcasted_iota(jnp.int32, (BLOCK, BLOCK), 0)
    earlier = lax.broadcasted_iota(jnp.int32, (BLOCK, BLOCK), 1)
    causal = later >= earlier
    first = lax.broadcasted_iota(jnp.int32, (BLOCK, 2 * HEAD_DIM), 1) < HEAD_DIM
    for pair in range(HEADS // 2):
        lanes = slice(pair * 2 * HEAD_DIM, (pair + 1) * 2 * HEAD_DIM)
        two = values[:, lanes]
        two_low = two.astype(bf16)
        parts = []
        for h in (2 * pair, 2 * pair + 1):
            away = columns[:, h * BLOCK : (h + 1) * BLOCK] - cum[h : h + 1, :]
            mixing = scores * jnp.exp(jnp.where(causal, away, -jnp.inf)) * steps[h : h + 1, :]
            parts.append(dot(mixing.astype(bf16), two_low, ((1,), (0,))))
        within = jnp.where(first, parts[0], parts[1])
        skip = jnp.where(first, skip_ref[2 * pair], skip_ref[2 * pair + 1])
        pre_ref[:, lanes] = within + skip * two


def row_kernel(got_ref, shard_ref, send_ref):
    start = shard_ref.shape[1]
    state = logs = None
    for k in range(got_ref.shape[0]):
        shard_ref[k] = got_ref[k, 0:start, :]
        more, step = take_state(got_ref, k, start)
        state, logs = (more, step) if state is None else (state * factor(step) + more, logs + step)
    for k in range(send_ref.shape[0]):
        put_state(send_ref, k, 0, state, logs)


def near_kernel(got_ref, send_ref, state_ref, logs_ref):
    here = lax.axis_index("zl")
    state = before = jnp.zeros((PAIR, STATE), f32)
    logs = passed = jnp.zeros((2, STATE), f32)
    for k in range(got_ref.shape[0]):
        more, step = take_state(got_ref, k, 0)
        state, logs = state * factor(step) + more, logs + step
        before, passed = jnp.where(k < here, state, before), jnp.where(k < here, logs, passed)
    state_ref[...] = before
    logs_ref[...] = passed
    for k in range(send_ref.shape[0]):
        put_state(send_ref, k, 0, state, logs)


def far_kernel(got_ref, state_ref, logs_ref, rows_ref, out_ref):
    here = lax.axis_index("zh")
    state = before = jnp.zeros((PAIR, STATE), f32)
    for k in range(got_ref.shape[0] - 1):
        more, step = take_state(got_ref, k, 0)
        state = state * factor(step) + more
        before = jnp.where(k < here, state, before)
    state = before * factor(logs_ref[...]) + state_ref[...]
    start = rows_ref.shape[1] - PAIR - TAIL
    for k in range(rows_ref.shape[0]):
        out_ref[k] = state.astype(bf16)
        if k + 1 < rows_ref.shape[0]:
            more, step = take_state(rows_ref, k, start)
            state = state * factor(step) + more


def gate_kernel(pre_ref, query_ref, cum_ref, inc_ref, gate_ref, gain_ref, w_ref, out_ref, w_room, sem):
    copy = pltpu.make_async_copy(w_ref, w_room, sem)
    copy.start()
    inc = inc_ref[...].reshape(WIDTH, STATE)
    arriving = dot(query_ref[...], inc, ((1,), (1,))) * spread(jnp.exp(cum_ref[...]), HEAD_DIM)
    gated = (pre_ref[...] + arriving) * silu(gate_ref[...].astype(f32))
    scale = lax.rsqrt(jnp.mean(gated * gated, axis=-1, keepdims=True) + EPSILON)
    heads_out = (gated * scale * gain_ref[...]).astype(bf16)
    copy.wait()
    out = dot(heads_out, w_room[...], ((1,), (0,))).astype(bf16)
    out_ref[...] = out.reshape(out_ref.shape)


def norm_kernel(got_ref, skip_ref, gain_ref, own_ref, copies_ref):
    total = got_ref[0].astype(f32)
    for k in range(1, got_ref.shape[0]):
        total = total + got_ref[k].astype(f32)
    own = (skip_ref[...].astype(f32) + total.astype(bf16).astype(f32)).astype(bf16)
    own_ref[...] = own
    wide = own.astype(f32)
    scale = lax.rsqrt(jnp.mean(wide * wide, axis=-1, keepdims=True) + EPSILON)
    normed = (wide * scale * gain_ref[...]).astype(bf16)
    for k in range(copies_ref.shape[0]):
        copies_ref[k] = normed


def mlp_kernel(rows_ref, w_ref, out_ref, w_room, sems):
    halves, shards, inner, slabs, each_depth, lanes = w_ref.shape
    pieces = sems.shape[1]
    take = shards // pieces
    size = take * inner * each_depth
    copies = []
    for j in range(pieces):
        for k in range(halves):
            part = pl.ds(j * take, take)
            copy = pltpu.make_async_copy(w_ref.at[k, part], w_room.at[k, part], sems.at[k, j])
            copy.start()
            copies.append(copy)

    def piece(k, j, first):
        parts = [w_room[k, j * take : (j + 1) * take, :, n, :, :] for n in (first, first + 1)]
        return jnp.concatenate([p.reshape(size, lanes) for p in parts], axis=1)

    count, each, depth = rows_ref.shape
    rows = rows_ref[...].reshape(count * each, depth)
    lifted = [None] * halves
    for j in range(pieces):
        for k in range(halves):
            copies[j * halves + k].wait()
            part = dot(rows[:, j * size : (j + 1) * size], piece(k, j, 0), ((1,), (0,)))
            lifted[k] = part if lifted[k] is None else lifted[k] + part
    hidden = []
    for k in range(halves):
        up = jnp.maximum(lifted[k], 0.0)
        hidden.append((up * up).astype(bf16))
    for j in range(pieces):
        total = None
        for k in range(halves):
            part = dot(hidden[k], piece(k, j, slabs // 2), ((1,), (1,)))
            total = part if total is None else total + part
        out_ref[:, :, j * size : (j + 1) * size] = total.astype(bf16).reshape(count, each, size)


def final_kernel(got_ref, own_ref, out_ref):
    total = got_ref[0].astype(f32)
    for k in range(1, got_ref.shape[0]):
        total = total + got_ref[k].astype(f32)
    out_ref[...] = (own_ref[...].astype(f32) + total.astype(bf16).astype(f32)).astype(bf16)


def per_device(
    skip_stream_entering,
    content_signal_matrix,
    writer_signal_matrix,
    reader_signal_matrix,
    multiplier_signal,
    interval_before_softplus,
    extra_log_shrink,
    log_forget_speed,
    content_filter_coefs,
    writer_filter_coefs,
    reader_filter_coefs,
    skip_path_factor,
    cluster_scaling_vector,
    blend_result_matrix,
    feature_blend_scaling,
    widening_matrix,
    narrowing_matrix,
):
    ny, nzl, nzh = (lax.axis_size(name) for name in ("y", "zl", "zh"))
    nsp = nzh * nzl * ny
    ntp = lax.axis_size("x") * lax.axis_size("c")
    nrows = ny * lax.axis_size("x")
    own_count, width = skip_stream_entering.shape
    depth, units = widening_matrix.shape
    shard = 2 * depth * units // ny // STATE

    rim = pl.pallas_call(
        first_kernel,
        grid=(1,),
        out_shape=shape((RIM, WIDTH + 2 * STATE), bf16),
        in_specs=[pl.BlockSpec((RIM, n), lambda i: (BLOCK // RIM - 1, 0)) for n in (WIDTH, STATE, STATE)],
        out_specs=pl.BlockSpec((RIM, WIDTH + 2 * STATE), lambda i: (0, 0)),
        interpret=INTERPRET,
    )(content_signal_matrix, writer_signal_matrix, reader_signal_matrix)
    rim = lax.ppermute(rim, SP, [(k, k + 1) for k in range(nsp - 1)])
    pre, query, cum, send = call(
        local_kernel,
        [
            shape((BLOCK, WIDTH), f32),
            shape((BLOCK, STATE), bf16),
            shape((HEADS, BLOCK), f32),
            shape((ny, shard + PAIR + TAIL, STATE), bf16),
        ],
        [VMEM] * 11 + [SMEM] * 2,
        [pltpu.VMEM((RIM + BLOCK, n), f32) for n in (WIDTH, STATE, STATE)],
    )(
        content_signal_matrix,
        writer_signal_matrix,
        reader_signal_matrix,
        near(rim),
        content_filter_coefs,
        writer_filter_coefs,
        reader_filter_coefs,
        interval_before_softplus,
        extra_log_shrink,
        widening_matrix,
        narrowing_matrix.T,
        log_forget_speed,
        skip_path_factor,
    )
    rows = near(exchange(send, "y"))
    parts, send = call(
        row_kernel,
        [jax.ShapeDtypeStruct((ny, shard, STATE), bf16), shape((nzl, PAIR + TAIL, STATE), bf16)],
        [VMEM],
    )(rows)
    weights = lax.all_gather(parts.reshape(ny * shard, STATE), ("c", "zh", "zl"), axis=0, tiled=True)
    weights = weights.reshape(-1, nzh * nzl, ny, shard // depth, depth, STATE)
    got = near(exchange(send, "zl"))
    send, state, logs = call(
        near_kernel,
        [shape((nzh, PAIR + TAIL, STATE), bf16), shape((PAIR, STATE), f32), shape((2, STATE), f32)],
        [VMEM],
    )(got)
    got = near(exchange(send, "zh"))
    before = call(far_kernel, shape((ny, PAIR, STATE), bf16), [VMEM] * 4)(got, near(state), near(logs), rows)
    incoming = exchange(before, "y")
    mixed = call(
        gate_kernel,
        shape((ntp, own_count, width), bf16),
        [VMEM] * 6 + [HBM],
        [pltpu.VMEM(blend_result_matrix.shape, bf16), pltpu.SemaphoreType.DMA(())],
    )(
        near(pre),
        near(query),
        near(cum),
        near(incoming),
        multiplier_signal,
        cluster_scaling_vector.reshape(1, -1),
        blend_result_matrix,
    )
    mixed = exchange(mixed, TP)
    own, copies = call(
        norm_kernel,
        [shape((own_count, width), bf16), shape((nrows, own_count, width), bf16)],
        [VMEM] * 3,
    )(near(mixed), skip_stream_entering, feature_blend_scaling.reshape(1, -1))
    rows = exchange(copies, ROWS)
    out = call(
        mlp_kernel,
        shape((nrows, own_count, width), bf16),
        [VMEM, HBM],
        [pltpu.VMEM(weights.shape, bf16), pltpu.SemaphoreType.DMA((weights.shape[0], 4))],
    )(near(rows), weights)
    out = exchange(out, ROWS)
    return call(final_kernel, jax.ShapeDtypeStruct((own_count, width), bf16), [VMEM] * 2)(near(out), near(own))


def solution(mesh):
    torus = Mesh(mesh.devices.reshape(4, 4, 4, 4, 2), SP + TP)
    placed = (
        P(SP + TP, None),
        P(SP, TP),
        P(SP, TP),
        P(SP, TP),
        P(SP, TP),
        P(TP, SP),
        P(TP, SP),
        P(TP),
        P(None, TP),
        P(None, TP),
        P(None, TP),
        P(TP),
        P(TP),
        P(TP, None),
        P(),
        P(SP, TP),
        P(TP, SP),
    )
    return jax.shard_map(
        per_device, mesh=torus, in_specs=placed, out_specs=P(SP + TP, None), check_vma=False
    )
```

```python
import functools

import jax
import jax.numpy as jnp
from jax import lax
from jax.experimental import pallas as pl
from jax.experimental.pallas import tpu as pltpu
from jax.sharding import Mesh
from jax.sharding import PartitionSpec as P

HEADS = 8
HEAD_DIM = 64
STATE = 128
BLOCK = 128
WIDTH = HEADS * HEAD_DIM
RIM = 8
TAIL = 16
NEAR = ("zl", "y")
SP = ("zh", "zl", "y")
TP = ("x", "c")
ROWS = ("y", "x")
EPSILON = 1e-05
INTERPRET = False
ROOM = pltpu.CompilerParams(vmem_limit_bytes=16 << 20)

f32 = jnp.float32
bf16 = jnp.bfloat16
VMEM = pl.BlockSpec(memory_space=pltpu.VMEM)
SMEM = pl.BlockSpec(memory_space=pltpu.SMEM)
HBM = pl.BlockSpec(memory_space=pl.ANY)


def call(kernel, outs, in_specs, scratch=(), **kw):
    single = not isinstance(outs, (list, tuple))
    return pl.pallas_call(
        kernel,
        out_shape=outs,
        in_specs=in_specs,
        out_specs=VMEM if single else [VMEM] * len(outs),
        scratch_shapes=list(scratch),
        interpret=INTERPRET,
        **kw,
    )


def shape(dims, kind):
    return jax.ShapeDtypeStruct(dims, kind) if INTERPRET else pltpu.VMEM(dims, kind)


def near(value):
    return value if INTERPRET else pltpu.with_memory_space_constraint(value, pltpu.VMEM)


def exchange(value, axes):
    return lax.all_to_all(value, axes, split_axis=0, concat_axis=0, tiled=True)


def dot(a, b, dims, **kw):
    return lax.dot_general(a, b, (dims, ((), ())), preferred_element_type=f32, **kw)


def spread(rows, width):
    head = lax.broadcasted_iota(jnp.int32, (HEADS, HEADS * width), 0)
    lane = lax.broadcasted_iota(jnp.int32, (HEADS, HEADS * width), 1)
    chosen = jnp.where(lane // width == head, 1.0, 0.0).astype(f32)
    return dot(rows, chosen, ((0,), (0,)), precision=lax.Precision.HIGHEST)


def silu(value):
    return value / (1.0 + jnp.exp(-value))


def convolve(src_ref, rim, taps_ref, room):
    room[0:RIM, :] = rim.astype(f32)
    room[RIM : RIM + BLOCK, :] = src_ref[...].astype(f32)
    taps = taps_ref[...].astype(f32)
    width = taps.shape[0]
    total = None
    for k in range(width):
        start = RIM - width + 1 + k
        term = room[start : start + BLOCK, :] * taps[k : k + 1, :]
        total = term if total is None else total + term
    return silu(total)


def put_state(ref, place, start, state, log):
    count = state.shape[0]
    ref[place, start : start + count, :] = state.astype(bf16)
    row = lax.broadcasted_iota(jnp.int32, (TAIL, STATE), 0)
    whole = jnp.broadcast_to(log, (TAIL, STATE))
    high = whole.astype(bf16).astype(f32)
    tail = jnp.where(row == 0, high, jnp.where(row == 1, whole - high, 0.0))
    ref[place, start + count : start + count + TAIL, :] = tail.astype(bf16)


def take_state(ref, place, start):
    end = ref.shape[1] - TAIL
    tail = ref[place, end : end + TAIL, :].astype(f32)
    return ref[place, start:end, :].astype(f32), tail[0:1, :] + tail[1:2, :]


def first_kernel(x_ref, b_ref, c_ref, rim_ref):
    rim_ref[:, 0:WIDTH] = x_ref[...]
    rim_ref[:, WIDTH : WIDTH + STATE] = b_ref[...]
    rim_ref[:, WIDTH + STATE : WIDTH + 2 * STATE] = c_ref[...]


def local_kernel(
    slices, x_ref, b_ref, c_ref, rim_ref, xt_ref, bt_ref, ct_ref, dt_ref, shrink_ref, up_ref, down_ref, speed_ref, skip_ref, w_ref,
    pre_ref, query_ref, cum_ref, send_ref, w_out, x_room, b_room, c_room, sem,
):
    copy = pltpu.make_async_copy(w_ref, w_out, sem)
    copy.start()
    values = convolve(x_ref, rim_ref[:, 0:WIDTH], xt_ref, x_room)
    keys = convolve(b_ref, rim_ref[:, WIDTH : WIDTH + STATE], bt_ref, b_room).astype(bf16)
    query = convolve(c_ref, rim_ref[:, WIDTH + STATE : WIDTH + 2 * STATE], ct_ref, c_room).astype(bf16)
    query_ref[...] = query
    before = dt_ref[...]
    steps = jnp.maximum(before, 0.0) + jnp.log1p(jnp.exp(-jnp.abs(before)))
    head = lax.broadcasted_iota(jnp.int32, (HEADS, BLOCK), 0)
    token = lax.broadcasted_iota(jnp.int32, (HEADS, BLOCK), 1)
    speed = jnp.zeros((HEADS, BLOCK), f32)
    for h in range(HEADS):
        speed = jnp.where(head == h, speed_ref[h], speed)
    cum = shrink_ref[...] - jnp.exp(speed) * steps
    reach = 1
    while reach < BLOCK:
        cum = cum + jnp.where(token >= reach, pltpu.roll(cum, reach, 1), 0.0)
        reach *= 2
    cum_ref[...] = cum
    last = cum[:, BLOCK - 1 : BLOCK]
    weight = steps * jnp.exp(last - cum)
    weighted = (values * spread(weight, HEAD_DIM)).astype(bf16)
    state = dot(weighted, keys, ((0,), (0,)))
    pieces = send_ref.shape[0]
    depth, units = up_ref.shape
    count = WIDTH // pieces
    slabs = units // slices // STATE
    for place in range(pieces):
        slab, k = divmod(place, slices)
        source = up_ref if slab < slabs else down_ref
        first_lane = (k * slabs + slab % slabs) * STATE
        send_ref[place, 0:depth, :] = source[:, first_lane : first_lane + STATE]
        h = place * count // HEAD_DIM
        put_state(send_ref, place, depth, state[place * count : (place + 1) * count, :], last[h : h + 1, :])
    scores = dot(query, keys, ((1,), (1,)))
    columns = spread(cum, BLOCK)
    later = lax.broadcasted_iota(jnp.int32, (BLOCK, BLOCK), 0)
    earlier = lax.broadcasted_iota(jnp.int32, (BLOCK, BLOCK), 1)
    causal = later >= earlier
    first = lax.broadcasted_iota(jnp.int32, (BLOCK, 2 * HEAD_DIM), 1) < HEAD_DIM
    for pair in range(HEADS // 2):
        lanes = slice(pair * 2 * HEAD_DIM, (pair + 1) * 2 * HEAD_DIM)
        two = values[:, lanes]
        two_low = two.astype(bf16)
        parts = []
        for h in (2 * pair, 2 * pair + 1):
            away = columns[:, h * BLOCK : (h + 1) * BLOCK] - cum[h : h + 1, :]
            mixing = scores * jnp.exp(jnp.where(causal, away, -jnp.inf)) * steps[h : h + 1, :]
            parts.append(dot(mixing.astype(bf16), two_low, ((1,), (0,))))
        within = jnp.where(first, parts[0], parts[1])
        skip = jnp.where(first, skip_ref[2 * pair], skip_ref[2 * pair + 1])
        pre_ref[:, lanes] = within + skip * two
    copy.wait()


def near_kernel(got_ref, shard_ref, send_ref):
    start = shard_ref.shape[1]
    state = log = None
    for k in range(got_ref.shape[0]):
        shard_ref[k] = got_ref[k, 0:start, :]
        more, step = take_state(got_ref, k, start)
        state, log = (more, step) if state is None else (state * jnp.exp(step) + more, log + step)
    for k in range(send_ref.shape[0]):
        put_state(send_ref, k, 0, state, log)


def far_kernel(got_ref, near_ref, out_ref):
    here = lax.axis_index("zh")
    count = out_ref.shape[1]
    state = before = jnp.zeros((count, STATE), f32)
    for k in range(got_ref.shape[0] - 1):
        more, step = take_state(got_ref, k, 0)
        state = state * jnp.exp(step) + more
        before = jnp.where(k < here, state, before)
    state = before
    start = near_ref.shape[1] - count - TAIL
    for k in range(near_ref.shape[0]):
        out_ref[k] = state.astype(bf16)
        if k + 1 < near_ref.shape[0]:
            more, step = take_state(near_ref, k, start)
            state = state * jnp.exp(step) + more


def gate_kernel(pre_ref, query_ref, cum_ref, inc_ref, gate_ref, gain_ref, w_ref, out_ref):
    inc = inc_ref[...].reshape(WIDTH, STATE)
    arriving = dot(query_ref[...], inc, ((1,), (1,))) * spread(jnp.exp(cum_ref[...]), HEAD_DIM)
    gated = (pre_ref[...] + arriving) * silu(gate_ref[...].astype(f32))
    scale = lax.rsqrt(jnp.mean(gated * gated, axis=-1, keepdims=True) + EPSILON)
    heads_out = (gated * scale * gain_ref[...]).astype(bf16)
    out = dot(heads_out, w_ref[...], ((1,), (0,))).astype(bf16)
    out_ref[...] = out.reshape(out_ref.shape)


def norm_kernel(got_ref, skip_ref, gain_ref, own_ref, copies_ref):
    total = got_ref[0].astype(f32)
    for k in range(1, got_ref.shape[0]):
        total = total + got_ref[k].astype(f32)
    own = (skip_ref[...].astype(f32) + total.astype(bf16).astype(f32)).astype(bf16)
    own_ref[...] = own
    wide = own.astype(f32)
    scale = lax.rsqrt(jnp.mean(wide * wide, axis=-1, keepdims=True) + EPSILON)
    normed = (wide * scale * gain_ref[...]).astype(bf16)
    for k in range(copies_ref.shape[0]):
        copies_ref[k] = normed


def mlp_kernel(rows_ref, w_ref, out_ref, w_room, sems):
    halves, pieces, slabs, size, lanes = w_ref.shape
    copies = []
    for j in range(pieces):
        for k in range(halves):
            copy = pltpu.make_async_copy(w_ref.at[k, j], w_room.at[k, j], sems.at[k, j])
            copy.start()
            copies.append(copy)

    def piece(k, j, first):
        return jnp.concatenate([w_room[k, j, n] for n in range(first, first + slabs // 2)], axis=1)

    count, each, depth = rows_ref.shape
    rows = rows_ref[...].reshape(count * each, depth)
    lifted = [None] * halves
    for j in range(pieces):
        for k in range(halves):
            copies[j * halves + k].wait()
            part = dot(rows[:, j * size : (j + 1) * size], piece(k, j, 0), ((1,), (0,)))
            lifted[k] = part if lifted[k] is None else lifted[k] + part
    hidden = []
    for k in range(halves):
        up = jnp.maximum(lifted[k], 0.0)
        hidden.append((up * up).astype(bf16))
    for j in range(pieces):
        total = None
        for k in range(halves):
            part = dot(hidden[k], piece(k, j, slabs // 2), ((1,), (1,)))
            total = part if total is None else total + part
        out_ref[:, :, j * size : (j + 1) * size] = total.astype(bf16).reshape(count, each, size)


def final_kernel(got_ref, own_ref, out_ref):
    total = got_ref[0].astype(f32)
    for k in range(1, got_ref.shape[0]):
        total = total + got_ref[k].astype(f32)
    out_ref[...] = (own_ref[...].astype(f32) + total.astype(bf16).astype(f32)).astype(bf16)


def per_device(
    skip_stream_entering,
    content_signal_matrix,
    writer_signal_matrix,
    reader_signal_matrix,
    multiplier_signal,
    interval_before_softplus,
    extra_log_shrink,
    log_forget_speed,
    content_filter_coefs,
    writer_filter_coefs,
    reader_filter_coefs,
    skip_path_factor,
    cluster_scaling_vector,
    blend_result_matrix,
    feature_blend_scaling,
    widening_matrix,
    narrowing_matrix,
):
    ny, nzl, nzh = (lax.axis_size(name) for name in ("y", "zl", "zh"))
    nsp = nzh * nzl * ny
    ntp = lax.axis_size("x") * lax.axis_size("c")
    nrows = ny * lax.axis_size("x")
    own_count, width = skip_stream_entering.shape
    depth, units = widening_matrix.shape
    pieces = nzl * ny
    count = WIDTH // pieces

    rim = pl.pallas_call(
        first_kernel,
        grid=(1,),
        out_shape=shape((RIM, WIDTH + 2 * STATE), bf16),
        in_specs=[pl.BlockSpec((RIM, n), lambda i: (BLOCK // RIM - 1, 0)) for n in (WIDTH, STATE, STATE)],
        out_specs=pl.BlockSpec((RIM, WIDTH + 2 * STATE), lambda i: (0, 0)),
        interpret=INTERPRET,
    )(content_signal_matrix, writer_signal_matrix, reader_signal_matrix)
    rim = lax.ppermute(rim, SP, [(k, k + 1) for k in range(nsp - 1)])
    pre, query, cum, send, projection = call(
        functools.partial(local_kernel, ny),
        [
            shape((BLOCK, WIDTH), f32),
            shape((BLOCK, STATE), bf16),
            shape((HEADS, BLOCK), f32),
            shape((pieces, depth + count + TAIL, STATE), bf16),
            shape(blend_result_matrix.shape, bf16),
        ],
        [VMEM] * 11 + [SMEM] * 2 + [HBM],
        [pltpu.VMEM((RIM + BLOCK, n), f32) for n in (WIDTH, STATE, STATE)] + [pltpu.SemaphoreType.DMA(())],
    )(
        content_signal_matrix,
        writer_signal_matrix,
        reader_signal_matrix,
        near(rim),
        content_filter_coefs,
        writer_filter_coefs,
        reader_filter_coefs,
        interval_before_softplus,
        extra_log_shrink,
        widening_matrix,
        narrowing_matrix.T,
        log_forget_speed,
        skip_path_factor,
        blend_result_matrix,
    )
    got = near(exchange(send, NEAR))
    parts, send = call(
        near_kernel,
        [jax.ShapeDtypeStruct((pieces, depth, STATE), bf16), shape((nzh, count + TAIL, STATE), bf16)],
        [VMEM],
        compiler_params=ROOM,
    )(got)
    weights = lax.all_gather(parts.reshape(pieces * depth, STATE), ("c", "zh", "zl"), axis=0, tiled=True)
    weights = weights.reshape(-1, nzh, nzl, pieces * depth, STATE)
    far = near(exchange(send, "zh"))
    before = call(far_kernel, shape((pieces, count, STATE), bf16), [VMEM] * 2, compiler_params=ROOM)(far, got)
    incoming = exchange(before, NEAR)
    mixed = call(
        gate_kernel,
        shape((ntp, own_count, width), bf16),
        [VMEM] * 7,
        compiler_params=ROOM,
    )(
        near(pre),
        near(query),
        near(cum),
        near(incoming),
        multiplier_signal,
        cluster_scaling_vector.reshape(1, -1),
        near(projection),
    )
    mixed = exchange(mixed, TP)
    own, copies = call(
        norm_kernel,
        [shape((own_count, width), bf16), shape((nrows, own_count, width), bf16)],
        [VMEM] * 3,
    )(near(mixed), skip_stream_entering, feature_blend_scaling.reshape(1, -1))
    rows = exchange(copies, ROWS)
    out = call(
        mlp_kernel,
        shape((nrows, own_count, width), bf16),
        [VMEM, HBM],
        [pltpu.VMEM(weights.shape, bf16), pltpu.SemaphoreType.DMA(weights.shape[:2])],
    )(near(rows), weights)
    out = exchange(out, ROWS)
    return call(final_kernel, jax.ShapeDtypeStruct((own_count, width), bf16), [VMEM] * 2)(near(out), near(own))


def solution(mesh):
    torus = Mesh(mesh.devices.reshape(4, 4, 4, 4, 2), SP + TP)
    placed = (
        P(SP + TP, None),
        P(SP, TP),
        P(SP, TP),
        P(SP, TP),
        P(SP, TP),
        P(TP, SP),
        P(TP, SP),
        P(TP),
        P(None, TP),
        P(None, TP),
        P(None, TP),
        P(TP),
        P(TP),
        P(TP, None),
        P(),
        P(SP, TP),
        P(TP, SP),
    )
    return jax.shard_map(
        per_device, mesh=torus, in_specs=placed, out_specs=P(SP + TP, None), check_vma=False
    )
```

```python
import jax
import jax.numpy as jnp
from jax import lax
from jax.experimental import pallas as pl
from jax.experimental.pallas import tpu as pltpu
from jax.sharding import Mesh
from jax.sharding import PartitionSpec as P

HEADS = 8
HEAD_DIM = 64
STATE = 128
BLOCK = 128
WIDTH = HEADS * HEAD_DIM
RIM = 8
TAIL = 16
NEAR = ("zl", "y")
SP = ("zh", "zl", "y")
TP = ("x", "c")
ROWS = ("y", "x")
EPSILON = 1e-05
INTERPRET = False
ROOM = pltpu.CompilerParams(vmem_limit_bytes=16 << 20)

f32 = jnp.float32
bf16 = jnp.bfloat16
VMEM = pl.BlockSpec(memory_space=pltpu.VMEM)
SMEM = pl.BlockSpec(memory_space=pltpu.SMEM)
HBM = pl.BlockSpec(memory_space=pl.ANY)


def call(kernel, outs, in_specs, scratch=(), **kw):
    single = not isinstance(outs, (list, tuple))
    return pl.pallas_call(
        kernel,
        out_shape=outs,
        in_specs=in_specs,
        out_specs=VMEM if single else [VMEM] * len(outs),
        scratch_shapes=list(scratch),
        interpret=INTERPRET,
        **kw,
    )


def shape(dims, kind):
    return jax.ShapeDtypeStruct(dims, kind) if INTERPRET else pltpu.VMEM(dims, kind)


def near(value):
    return value if INTERPRET else pltpu.with_memory_space_constraint(value, pltpu.VMEM)


def exchange(value, axes):
    return lax.all_to_all(value, axes, split_axis=0, concat_axis=0, tiled=True)


def dot(a, b, dims, **kw):
    return lax.dot_general(a, b, (dims, ((), ())), preferred_element_type=f32, **kw)


def spread(rows, width):
    head = lax.broadcasted_iota(jnp.int32, (HEADS, HEADS * width), 0)
    lane = lax.broadcasted_iota(jnp.int32, (HEADS, HEADS * width), 1)
    chosen = jnp.where(lane // width == head, 1.0, 0.0).astype(f32)
    return dot(rows, chosen, ((0,), (0,)), precision=lax.Precision.HIGHEST)


def silu(value):
    return value / (1.0 + jnp.exp(-value))


def convolve(src_ref, rim, taps_ref, room):
    room[0:RIM, :] = rim.astype(f32)
    room[RIM : RIM + BLOCK, :] = src_ref[...].astype(f32)
    taps = taps_ref[...].astype(f32)
    width = taps.shape[0]
    total = None
    for k in range(width):
        start = RIM - width + 1 + k
        term = room[start : start + BLOCK, :] * taps[k : k + 1, :]
        total = term if total is None else total + term
    return silu(total)


def put_state(ref, place, start, state, log):
    count = state.shape[0]
    ref[place, start : start + count, :] = state.astype(bf16)
    row = lax.broadcasted_iota(jnp.int32, (TAIL, STATE), 0)
    whole = jnp.broadcast_to(log, (TAIL, STATE))
    high = whole.astype(bf16).astype(f32)
    tail = jnp.where(row == 0, high, jnp.where(row == 1, whole - high, 0.0))
    ref[place, start + count : start + count + TAIL, :] = tail.astype(bf16)


def take_state(ref, place, start):
    end = ref.shape[1] - TAIL
    tail = ref[place, end : end + TAIL, :].astype(f32)
    return ref[place, start:end, :].astype(f32), tail[0:1, :] + tail[1:2, :]


def rim_kernel(x_ref, b_ref, c_ref, rim_ref):
    rim_ref[:, 0:WIDTH] = x_ref[...]
    rim_ref[:, WIDTH : WIDTH + STATE] = b_ref[...]
    rim_ref[:, WIDTH + STATE : WIDTH + 2 * STATE] = c_ref[...]


def pack_kernel(up_ref, down_ref, mine_ref):
    depth, units = up_ref.shape
    slices = mine_ref.shape[0]
    slabs = units // slices // STATE
    for k in range(slices):
        for j in range(slabs):
            lanes = slice((k * slabs + j) * STATE, (k * slabs + j + 1) * STATE)
            mine_ref[k, j * depth : (j + 1) * depth, :] = up_ref[:, lanes]
            mine_ref[k, (slabs + j) * depth : (slabs + j + 1) * depth, :] = down_ref[:, lanes]


def local_kernel(
    x_ref, b_ref, c_ref, rim_ref, xt_ref, bt_ref, ct_ref, dt_ref, shrink_ref, speed_ref, skip_ref, w_ref,
    pre_ref, query_ref, cum_ref, send_ref, w_out, x_room, b_room, c_room, sem,
):
    copy = pltpu.make_async_copy(w_ref, w_out, sem)
    copy.start()
    values = convolve(x_ref, rim_ref[:, 0:WIDTH], xt_ref, x_room)
    keys = convolve(b_ref, rim_ref[:, WIDTH : WIDTH + STATE], bt_ref, b_room).astype(bf16)
    query = convolve(c_ref, rim_ref[:, WIDTH + STATE : WIDTH + 2 * STATE], ct_ref, c_room).astype(bf16)
    query_ref[...] = query
    before = dt_ref[...]
    steps = jnp.maximum(before, 0.0) + jnp.log1p(jnp.exp(-jnp.abs(before)))
    head = lax.broadcasted_iota(jnp.int32, (HEADS, BLOCK), 0)
    token = lax.broadcasted_iota(jnp.int32, (HEADS, BLOCK), 1)
    speed = jnp.zeros((HEADS, BLOCK), f32)
    for h in range(HEADS):
        speed = jnp.where(head == h, speed_ref[h], speed)
    cum = shrink_ref[...] - jnp.exp(speed) * steps
    reach = 1
    while reach < BLOCK:
        cum = cum + jnp.where(token >= reach, pltpu.roll(cum, reach, 1), 0.0)
        reach *= 2
    cum_ref[...] = cum
    last = cum[:, BLOCK - 1 : BLOCK]
    weight = steps * jnp.exp(last - cum)
    weighted = (values * spread(weight, HEAD_DIM)).astype(bf16)
    state = dot(weighted, keys, ((0,), (0,)))
    pieces = send_ref.shape[0]
    count = WIDTH // pieces
    for place in range(pieces):
        h = place * count // HEAD_DIM
        put_state(send_ref, place, 0, state[place * count : (place + 1) * count, :], last[h : h + 1, :])
    scores = dot(query, keys, ((1,), (1,)))
    columns = spread(cum, BLOCK)
    later = lax.broadcasted_iota(jnp.int32, (BLOCK, BLOCK), 0)
    earlier = lax.broadcasted_iota(jnp.int32, (BLOCK, BLOCK), 1)
    causal = later >= earlier
    first = lax.broadcasted_iota(jnp.int32, (BLOCK, 2 * HEAD_DIM), 1) < HEAD_DIM
    for pair in range(HEADS // 2):
        lanes = slice(pair * 2 * HEAD_DIM, (pair + 1) * 2 * HEAD_DIM)
        two = values[:, lanes]
        two_low = two.astype(bf16)
        parts = []
        for h in (2 * pair, 2 * pair + 1):
            away = columns[:, h * BLOCK : (h + 1) * BLOCK] - cum[h : h + 1, :]
            mixing = scores * jnp.exp(jnp.where(causal, away, -jnp.inf)) * steps[h : h + 1, :]
            parts.append(dot(mixing.astype(bf16), two_low, ((1,), (0,))))
        within = jnp.where(first, parts[0], parts[1])
        skip = jnp.where(first, skip_ref[2 * pair], skip_ref[2 * pair + 1])
        pre_ref[:, lanes] = within + skip * two
    copy.wait()


def near_kernel(got_ref, send_ref):
    state = log = None
    for k in range(got_ref.shape[0]):
        more, step = take_state(got_ref, k, 0)
        state, log = (more, step) if state is None else (state * jnp.exp(step) + more, log + step)
    for k in range(send_ref.shape[0]):
        put_state(send_ref, k, 0, state, log)


def far_kernel(got_ref, near_ref, out_ref):
    here = lax.axis_index("zh")
    count = out_ref.shape[1]
    state = before = jnp.zeros((count, STATE), f32)
    for k in range(got_ref.shape[0] - 1):
        more, step = take_state(got_ref, k, 0)
        state = state * jnp.exp(step) + more
        before = jnp.where(k < here, state, before)
    state = before
    for k in range(near_ref.shape[0]):
        out_ref[k] = state.astype(bf16)
        if k + 1 < near_ref.shape[0]:
            more, step = take_state(near_ref, k, 0)
            state = state * jnp.exp(step) + more


def gate_kernel(pre_ref, query_ref, cum_ref, inc_ref, gate_ref, gain_ref, w_ref, out_ref):
    inc = inc_ref[...].reshape(WIDTH, STATE)
    arriving = dot(query_ref[...], inc, ((1,), (1,))) * spread(jnp.exp(cum_ref[...]), HEAD_DIM)
    gated = (pre_ref[...] + arriving) * silu(gate_ref[...].astype(f32))
    scale = lax.rsqrt(jnp.mean(gated * gated, axis=-1, keepdims=True) + EPSILON)
    heads_out = (gated * scale * gain_ref[...]).astype(bf16)
    out = dot(heads_out, w_ref[...], ((1,), (0,))).astype(bf16)
    out_ref[...] = out.reshape(out_ref.shape)


def norm_kernel(got_ref, skip_ref, gain_ref, own_ref, copies_ref):
    total = got_ref[0].astype(f32)
    for k in range(1, got_ref.shape[0]):
        total = total + got_ref[k].astype(f32)
    own = (skip_ref[...].astype(f32) + total.astype(bf16).astype(f32)).astype(bf16)
    own_ref[...] = own
    wide = own.astype(f32)
    scale = lax.rsqrt(jnp.mean(wide * wide, axis=-1, keepdims=True) + EPSILON)
    normed = (wide * scale * gain_ref[...]).astype(bf16)
    for k in range(copies_ref.shape[0]):
        copies_ref[k] = normed


def mlp_kernel(rows_ref, w_ref, out_ref, w_room, sems):
    halves, shards, inner, slabs, each_depth, lanes = w_ref.shape
    pieces = sems.shape[1]
    take = shards // pieces
    size = take * inner * each_depth
    copies = []
    for j in range(pieces):
        for k in range(halves):
            part = pl.ds(j * take, take)
            copy = pltpu.make_async_copy(w_ref.at[k, part], w_room.at[k, part], sems.at[k, j])
            copy.start()
            copies.append(copy)

    def piece(k, j, first):
        parts = [w_room[k, j * take : (j + 1) * take, :, n, :, :] for n in (first, first + 1)]
        return jnp.concatenate([p.reshape(size, lanes) for p in parts], axis=1)

    count, each, depth = rows_ref.shape
    rows = rows_ref[...].reshape(count * each, depth)
    lifted = [None] * halves
    for j in range(pieces):
        for k in range(halves):
            copies[j * halves + k].wait()
            part = dot(rows[:, j * size : (j + 1) * size], piece(k, j, 0), ((1,), (0,)))
            lifted[k] = part if lifted[k] is None else lifted[k] + part
    hidden = []
    for k in range(halves):
        up = jnp.maximum(lifted[k], 0.0)
        hidden.append((up * up).astype(bf16))
    for j in range(pieces):
        total = None
        for k in range(halves):
            part = dot(hidden[k], piece(k, j, slabs // 2), ((1,), (1,)))
            total = part if total is None else total + part
        out_ref[:, :, j * size : (j + 1) * size] = total.astype(bf16).reshape(count, each, size)


def final_kernel(got_ref, own_ref, out_ref):
    total = got_ref[0].astype(f32)
    for k in range(1, got_ref.shape[0]):
        total = total + got_ref[k].astype(f32)
    out_ref[...] = (own_ref[...].astype(f32) + total.astype(bf16).astype(f32)).astype(bf16)


def layer(
    skip_stream_entering,
    content_signal_matrix,
    writer_signal_matrix,
    reader_signal_matrix,
    multiplier_signal,
    interval_before_softplus,
    extra_log_shrink,
    log_forget_speed,
    content_filter_coefs,
    writer_filter_coefs,
    reader_filter_coefs,
    skip_path_factor,
    cluster_scaling_vector,
    blend_result_matrix,
    feature_blend_scaling,
    widening_matrix,
    narrowing_matrix,
):
    ny, nzl, nzh = (lax.axis_size(name) for name in ("y", "zl", "zh"))
    nsp = nzh * nzl * ny
    ntp = lax.axis_size("x") * lax.axis_size("c")
    nrows = ny * lax.axis_size("x")
    own_count, width = skip_stream_entering.shape
    depth, units = widening_matrix.shape
    pieces = nzl * ny
    count = WIDTH // pieces
    shard = 2 * depth * units // ny // STATE

    rim = pl.pallas_call(
        rim_kernel,
        grid=(1,),
        out_shape=shape((RIM, WIDTH + 2 * STATE), bf16),
        in_specs=[pl.BlockSpec((RIM, n), lambda i: (BLOCK // RIM - 1, 0)) for n in (WIDTH, STATE, STATE)],
        out_specs=pl.BlockSpec((RIM, WIDTH + 2 * STATE), lambda i: (0, 0)),
        interpret=INTERPRET,
    )(content_signal_matrix, writer_signal_matrix, reader_signal_matrix)
    rim = lax.ppermute(rim, SP, [(k, k + 1) for k in range(nsp - 1)])
    mine = call(pack_kernel, shape((ny, shard, STATE), bf16), [VMEM] * 2)(
        widening_matrix, narrowing_matrix.T
    )
    parts = exchange(mine, "y")
    weights = lax.all_gather(parts.reshape(ny * shard, STATE), ("c", "zh", "zl"), axis=0, tiled=True)
    weights = weights.reshape(-1, nzh * nzl, ny, shard // depth, depth, STATE)
    rim, parts = lax.optimization_barrier((rim, parts))
    pre, query, cum, send, projection = call(
        local_kernel,
        [
            shape((BLOCK, WIDTH), f32),
            shape((BLOCK, STATE), bf16),
            shape((HEADS, BLOCK), f32),
            shape((pieces, count + TAIL, STATE), bf16),
            shape(blend_result_matrix.shape, bf16),
        ],
        [VMEM] * 9 + [SMEM] * 2 + [HBM],
        [pltpu.VMEM((RIM + BLOCK, n), f32) for n in (WIDTH, STATE, STATE)] + [pltpu.SemaphoreType.DMA(())],
    )(
        content_signal_matrix,
        writer_signal_matrix,
        reader_signal_matrix,
        near(rim),
        content_filter_coefs,
        writer_filter_coefs,
        reader_filter_coefs,
        interval_before_softplus,
        extra_log_shrink,
        log_forget_speed,
        skip_path_factor,
        blend_result_matrix,
    )
    got = near(exchange(send, NEAR))
    send = call(near_kernel, shape((nzh, count + TAIL, STATE), bf16), [VMEM], compiler_params=ROOM)(got)
    far = near(exchange(send, "zh"))
    before = call(far_kernel, shape((pieces, count, STATE), bf16), [VMEM] * 2, compiler_params=ROOM)(far, got)
    incoming = exchange(before, NEAR)
    mixed = call(
        gate_kernel,
        shape((ntp, own_count, width), bf16),
        [VMEM] * 7,
        compiler_params=ROOM,
    )(
        near(pre),
        near(query),
        near(cum),
        near(incoming),
        multiplier_signal,
        cluster_scaling_vector.reshape(1, -1),
        near(projection),
    )
    mixed = exchange(mixed, TP)
    own, copies = call(
        norm_kernel,
        [shape((own_count, width), bf16), shape((nrows, own_count, width), bf16)],
        [VMEM] * 3,
    )(near(mixed), skip_stream_entering, feature_blend_scaling.reshape(1, -1))
    rows = exchange(copies, ROWS)
    out = call(
        mlp_kernel,
        shape((nrows, own_count, width), bf16),
        [VMEM, HBM],
        [pltpu.VMEM(weights.shape, bf16), pltpu.SemaphoreType.DMA((weights.shape[0], 4))],
    )(near(rows), weights)
    out = exchange(out, ROWS)
    return call(final_kernel, jax.ShapeDtypeStruct((own_count, width), bf16), [VMEM] * 2)(near(out), near(own))


def solution(mesh):
    torus = Mesh(mesh.devices.reshape(4, 4, 4, 4, 2), SP + TP)
    placed = (
        P(SP + TP, None),
        P(SP, TP),
        P(SP, TP),
        P(SP, TP),
        P(SP, TP),
        P(TP, SP),
        P(TP, SP),
        P(TP),
        P(None, TP),
        P(None, TP),
        P(None, TP),
        P(TP),
        P(TP),
        P(TP, None),
        P(),
        P(SP, TP),
        P(TP, SP),
    )
    return jax.shard_map(layer, mesh=torus, in_specs=placed, out_specs=P(SP + TP, None), check_vma=False)
```

```python
import jax
import jax.numpy as jnp
from jax import lax
from jax.experimental import pallas as pl
from jax.experimental.pallas import tpu as pltpu
from jax.sharding import Mesh
from jax.sharding import PartitionSpec as P

HEADS = 8
HEAD_DIM = 64
STATE = 128
BLOCK = 128
WIDTH = HEADS * HEAD_DIM
RIM = 8
PAIR = 2 * HEAD_DIM
TAIL = 16
SP = ("zh", "zl", "y")
TP = ("x", "c")
ROWS = ("y", "x")
EPSILON = 1e-05
INTERPRET = False
ROOM = pltpu.CompilerParams(vmem_limit_bytes=16 << 20)

f32 = jnp.float32
bf16 = jnp.bfloat16
VMEM = pl.BlockSpec(memory_space=pltpu.VMEM)
SMEM = pl.BlockSpec(memory_space=pltpu.SMEM)
HBM = pl.BlockSpec(memory_space=pl.ANY)


def call(kernel, outs, in_specs, scratch=(), **kw):
    single = not isinstance(outs, (list, tuple))
    return pl.pallas_call(
        kernel,
        out_shape=outs,
        in_specs=in_specs,
        out_specs=VMEM if single else [VMEM] * len(outs),
        scratch_shapes=list(scratch),
        interpret=INTERPRET,
        **kw,
    )


def shape(dims, kind):
    return jax.ShapeDtypeStruct(dims, kind) if INTERPRET else pltpu.VMEM(dims, kind)


def near(value):
    return value if INTERPRET else pltpu.with_memory_space_constraint(value, pltpu.VMEM)


def exchange(value, axes):
    return lax.all_to_all(value, axes, split_axis=0, concat_axis=0, tiled=True)


def dot(a, b, dims, **kw):
    return lax.dot_general(a, b, (dims, ((), ())), preferred_element_type=f32, **kw)


def spread(rows, width):
    head = lax.broadcasted_iota(jnp.int32, (HEADS, HEADS * width), 0)
    lane = lax.broadcasted_iota(jnp.int32, (HEADS, HEADS * width), 1)
    chosen = jnp.where(lane // width == head, 1.0, 0.0).astype(f32)
    return dot(rows, chosen, ((0,), (0,)), precision=lax.Precision.HIGHEST)


def silu(value):
    return value / (1.0 + jnp.exp(-value))


def convolve(room, taps_ref, count):
    taps = taps_ref[...].astype(f32)
    width = taps.shape[0]
    total = None
    for k in range(width):
        start = RIM - width + 1 + k
        term = room[start : start + count, :] * taps[k : k + 1, :]
        total = term if total is None else total + term
    return total


def put_state(ref, place, start, state, logs):
    ref[place, start : start + PAIR, :] = state.astype(bf16)
    row = lax.broadcasted_iota(jnp.int32, (TAIL, STATE), 0)
    tail = jnp.zeros((TAIL, STATE), f32)
    for h in range(2):
        whole = jnp.broadcast_to(logs[h : h + 1, :], (TAIL, STATE))
        high = whole.astype(bf16).astype(f32)
        tail = jnp.where(row == 2 * h, high, jnp.where(row == 2 * h + 1, whole - high, tail))
    ref[place, start + PAIR : start + PAIR + TAIL, :] = tail.astype(bf16)


def take_state(ref, place, start):
    state = ref[place, start : start + PAIR, :].astype(f32)
    tail = ref[place, start + PAIR : start + PAIR + TAIL, :].astype(f32)
    return state, jnp.concatenate([tail[2 * h : 2 * h + 1, :] + tail[2 * h + 1 : 2 * h + 2, :] for h in range(2)], axis=0)


def factor(logs):
    grown = jnp.exp(logs)
    return jnp.concatenate([jnp.broadcast_to(grown[h : h + 1, :], (HEAD_DIM, STATE)) for h in range(2)], axis=0)


def first_kernel(x_ref, b_ref, c_ref, rim_ref):
    rim_ref[:, 0:WIDTH] = x_ref[...]
    rim_ref[:, WIDTH : WIDTH + STATE] = b_ref[...]
    rim_ref[:, WIDTH + STATE : WIDTH + 2 * STATE] = c_ref[...]


def early_kernel(
    x_ref, b_ref, c_ref, xt_ref, bt_ref, ct_ref, dt_ref, shrink_ref, speed_ref,
    x_out, b_out, c_out, cum_ref, weight_ref, mask_ref, x_room, b_room, c_room,
):
    for src_ref, taps_ref, out_ref, room in (
        (x_ref, xt_ref, x_out, x_room), (b_ref, bt_ref, b_out, b_room), (c_ref, ct_ref, c_out, c_room)
    ):
        room[0:RIM, :] = jnp.zeros((RIM, room.shape[1]), f32)
        room[RIM : RIM + BLOCK, :] = src_ref[...].astype(f32)
        out_ref[...] = convolve(room, taps_ref, BLOCK)
    before = dt_ref[...]
    steps = jnp.maximum(before, 0.0) + jnp.log1p(jnp.exp(-jnp.abs(before)))
    head = lax.broadcasted_iota(jnp.int32, (HEADS, BLOCK), 0)
    token = lax.broadcasted_iota(jnp.int32, (HEADS, BLOCK), 1)
    speed = jnp.zeros((HEADS, BLOCK), f32)
    for h in range(HEADS):
        speed = jnp.where(head == h, speed_ref[h], speed)
    cum = shrink_ref[...] - jnp.exp(speed) * steps
    reach = 1
    while reach < BLOCK:
        cum = cum + jnp.where(token >= reach, pltpu.roll(cum, reach, 1), 0.0)
        reach *= 2
    cum_ref[...] = cum
    weight_ref[...] = spread(steps * jnp.exp(cum[:, BLOCK - 1 : BLOCK] - cum), HEAD_DIM)
    columns = spread(cum, BLOCK)
    later = lax.broadcasted_iota(jnp.int32, (BLOCK, BLOCK), 0)
    earlier = lax.broadcasted_iota(jnp.int32, (BLOCK, BLOCK), 1)
    causal = later >= earlier
    for h in range(HEADS):
        away = columns[:, h * BLOCK : (h + 1) * BLOCK] - cum[h : h + 1, :]
        mask_ref[h] = jnp.exp(jnp.where(causal, away, -jnp.inf)) * steps[h : h + 1, :]


def local_kernel(
    x_ref, b_ref, c_ref, rim_ref, xt_ref, bt_ref, ct_ref, x_sum, b_sum, c_sum, cum_ref, weight_ref, mask_ref,
    up_ref, down_ref, skip_ref, w_ref,
    pre_ref, query_ref, send_ref, w_out, x_room, b_room, c_room, sem,
):
    copy = pltpu.make_async_copy(w_ref, w_out, sem)
    copy.start()
    rows = []
    lane = 0
    for src_ref, taps_ref, sum_ref, room in (
        (x_ref, xt_ref, x_sum, x_room), (b_ref, bt_ref, b_sum, b_room), (c_ref, ct_ref, c_sum, c_room)
    ):
        room[0:RIM, :] = rim_ref[:, lane : lane + room.shape[1]].astype(f32)
        room[RIM : 2 * RIM, :] = src_ref[...].astype(f32)
        lane += room.shape[1]
        head = convolve(room, taps_ref, RIM)
        rows.append(silu(jnp.concatenate([head, sum_ref[RIM:BLOCK, :]], axis=0)))
    values, keys, query = rows[0], rows[1].astype(bf16), rows[2].astype(bf16)
    query_ref[...] = query
    last = cum_ref[:, BLOCK - 1 : BLOCK]
    state = dot((values * weight_ref[...]).astype(bf16), keys, ((0,), (0,)))
    pieces = send_ref.shape[0]
    depth, units = up_ref.shape
    slabs = units // pieces // STATE
    for k in range(pieces):
        for j in range(slabs):
            lanes = slice((k * slabs + j) * STATE, (k * slabs + j + 1) * STATE)
            send_ref[k, j * depth : (j + 1) * depth, :] = up_ref[:, lanes]
            send_ref[k, (slabs + j) * depth : (slabs + j + 1) * depth, :] = down_ref[:, lanes]
        put_state(send_ref, k, 2 * slabs * depth, state[k * PAIR : (k + 1) * PAIR, :], last[2 * k : 2 * k + 2, :])
    scores = dot(query, keys, ((1,), (1,)))
    first = lax.broadcasted_iota(jnp.int32, (BLOCK, 2 * HEAD_DIM), 1) < HEAD_DIM
    for pair in range(HEADS // 2):
        lanes = slice(pair * 2 * HEAD_DIM, (pair + 1) * 2 * HEAD_DIM)
        two = values[:, lanes]
        two_low = two.astype(bf16)
        parts = []
        for h in (2 * pair, 2 * pair + 1):
            mixing = scores * mask_ref[h]
            parts.append(dot(mixing.astype(bf16), two_low, ((1,), (0,))))
        within = jnp.where(first, parts[0], parts[1])
        skip = jnp.where(first, skip_ref[2 * pair], skip_ref[2 * pair + 1])
        pre_ref[:, lanes] = within + skip * two
    copy.wait()


def row_kernel(got_ref, shard_ref, send_ref):
    start = shard_ref.shape[1]
    state = logs = None
    for k in range(got_ref.shape[0]):
        shard_ref[k] = got_ref[k, 0:start, :]
        more, step = take_state(got_ref, k, start)
        state, logs = (more, step) if state is None else (state * factor(step) + more, logs + step)
    for k in range(send_ref.shape[0]):
        put_state(send_ref, k, 0, state, logs)


def near_kernel(got_ref, send_ref, state_ref, logs_ref):
    here = lax.axis_index("zl")
    state = before = jnp.zeros((PAIR, STATE), f32)
    logs = passed = jnp.zeros((2, STATE), f32)
    for k in range(got_ref.shape[0]):
        more, step = take_state(got_ref, k, 0)
        state, logs = state * factor(step) + more, logs + step
        before, passed = jnp.where(k < here, state, before), jnp.where(k < here, logs, passed)
    state_ref[...] = before
    logs_ref[...] = passed
    for k in range(send_ref.shape[0]):
        put_state(send_ref, k, 0, state, logs)


def far_kernel(got_ref, state_ref, logs_ref, rows_ref, out_ref):
    here = lax.axis_index("zh")
    state = before = jnp.zeros((PAIR, STATE), f32)
    for k in range(got_ref.shape[0] - 1):
        more, step = take_state(got_ref, k, 0)
        state = state * factor(step) + more
        before = jnp.where(k < here, state, before)
    state = before * factor(logs_ref[...]) + state_ref[...]
    start = rows_ref.shape[1] - PAIR - TAIL
    for k in range(rows_ref.shape[0]):
        out_ref[k] = state.astype(bf16)
        if k + 1 < rows_ref.shape[0]:
            more, step = take_state(rows_ref, k, start)
            state = state * factor(step) + more


def gate_kernel(pre_ref, query_ref, cum_ref, inc_ref, gate_ref, gain_ref, w_ref, out_ref):
    inc = inc_ref[...].reshape(WIDTH, STATE)
    arriving = dot(query_ref[...], inc, ((1,), (1,))) * spread(jnp.exp(cum_ref[...]), HEAD_DIM)
    gated = (pre_ref[...] + arriving) * silu(gate_ref[...].astype(f32))
    scale = lax.rsqrt(jnp.mean(gated * gated, axis=-1, keepdims=True) + EPSILON)
    heads_out = (gated * scale * gain_ref[...]).astype(bf16)
    out = dot(heads_out, w_ref[...], ((1,), (0,))).astype(bf16)
    out_ref[...] = out.reshape(out_ref.shape)


def norm_kernel(got_ref, skip_ref, gain_ref, own_ref, copies_ref):
    total = got_ref[0].astype(f32)
    for k in range(1, got_ref.shape[0]):
        total = total + got_ref[k].astype(f32)
    own = (skip_ref[...].astype(f32) + total.astype(bf16).astype(f32)).astype(bf16)
    own_ref[...] = own
    wide = own.astype(f32)
    scale = lax.rsqrt(jnp.mean(wide * wide, axis=-1, keepdims=True) + EPSILON)
    normed = (wide * scale * gain_ref[...]).astype(bf16)
    for k in range(copies_ref.shape[0]):
        copies_ref[k] = normed


def mlp_kernel(rows_ref, w_ref, out_ref, w_room, sems):
    halves, shards, inner, slabs, each_depth, lanes = w_ref.shape
    pieces = sems.shape[1]
    take = shards // pieces
    size = take * inner * each_depth
    copies = []
    for j in range(pieces):
        for k in range(halves):
            part = pl.ds(j * take, take)
            copy = pltpu.make_async_copy(w_ref.at[k, part], w_room.at[k, part], sems.at[k, j])
            copy.start()
            copies.append(copy)

    def piece(k, j, first):
        parts = [w_room[k, j * take : (j + 1) * take, :, n, :, :] for n in (first, first + 1)]
        return jnp.concatenate([p.reshape(size, lanes) for p in parts], axis=1)

    count, each, depth = rows_ref.shape
    rows = rows_ref[...].reshape(count * each, depth)
    lifted = [None] * halves
    for j in range(pieces):
        for k in range(halves):
            copies[j * halves + k].wait()
            part = dot(rows[:, j * size : (j + 1) * size], piece(k, j, 0), ((1,), (0,)))
            lifted[k] = part if lifted[k] is None else lifted[k] + part
    hidden = []
    for k in range(halves):
        up = jnp.maximum(lifted[k], 0.0)
        hidden.append((up * up).astype(bf16))
    for j in range(pieces):
        total = None
        for k in range(halves):
            part = dot(hidden[k], piece(k, j, slabs // 2), ((1,), (1,)))
            total = part if total is None else total + part
        out_ref[:, :, j * size : (j + 1) * size] = total.astype(bf16).reshape(count, each, size)


def final_kernel(got_ref, own_ref, out_ref):
    total = got_ref[0].astype(f32)
    for k in range(1, got_ref.shape[0]):
        total = total + got_ref[k].astype(f32)
    out_ref[...] = (own_ref[...].astype(f32) + total.astype(bf16).astype(f32)).astype(bf16)


def layer(
    skip_stream_entering,
    content_signal_matrix,
    writer_signal_matrix,
    reader_signal_matrix,
    multiplier_signal,
    interval_before_softplus,
    extra_log_shrink,
    log_forget_speed,
    content_filter_coefs,
    writer_filter_coefs,
    reader_filter_coefs,
    skip_path_factor,
    cluster_scaling_vector,
    blend_result_matrix,
    feature_blend_scaling,
    widening_matrix,
    narrowing_matrix,
):
    ny, nzl, nzh = (lax.axis_size(name) for name in ("y", "zl", "zh"))
    nsp = nzh * nzl * ny
    ntp = lax.axis_size("x") * lax.axis_size("c")
    nrows = ny * lax.axis_size("x")
    own_count, width = skip_stream_entering.shape
    depth, units = widening_matrix.shape
    shard = 2 * depth * units // ny // STATE

    rim = pl.pallas_call(
        first_kernel,
        grid=(1,),
        out_shape=shape((RIM, WIDTH + 2 * STATE), bf16),
        in_specs=[pl.BlockSpec((RIM, n), lambda i: (BLOCK // RIM - 1, 0)) for n in (WIDTH, STATE, STATE)],
        out_specs=pl.BlockSpec((RIM, WIDTH + 2 * STATE), lambda i: (0, 0)),
        interpret=INTERPRET,
    )(content_signal_matrix, writer_signal_matrix, reader_signal_matrix)
    rim = lax.ppermute(rim, SP, [(k, k + 1) for k in range(nsp - 1)])
    *sums, cum, weight, mask = call(
        early_kernel,
        [
            shape((BLOCK, WIDTH), f32),
            shape((BLOCK, STATE), f32),
            shape((BLOCK, STATE), f32),
            shape((HEADS, BLOCK), f32),
            shape((BLOCK, WIDTH), f32),
            shape((HEADS, BLOCK, BLOCK), f32),
        ],
        [VMEM] * 8 + [SMEM],
        [pltpu.VMEM((RIM + BLOCK, n), f32) for n in (WIDTH, STATE, STATE)],
    )(
        content_signal_matrix,
        writer_signal_matrix,
        reader_signal_matrix,
        content_filter_coefs,
        writer_filter_coefs,
        reader_filter_coefs,
        interval_before_softplus,
        extra_log_shrink,
        log_forget_speed,
    )

    def whole(value):
        zeros = (0,) * value.ndim
        return pl.BlockSpec(value.shape, lambda i: zeros)

    head_rows = (content_signal_matrix, writer_signal_matrix, reader_signal_matrix)
    taps = (content_filter_coefs, writer_filter_coefs, reader_filter_coefs)
    kept = [near(value) for value in (*sums, cum, weight, mask)]
    outs = [
        shape((BLOCK, WIDTH), f32),
        jax.ShapeDtypeStruct((BLOCK, STATE), bf16),
        shape((ny, shard + PAIR + TAIL, STATE), bf16),
        shape(blend_result_matrix.shape, bf16),
    ]
    narrowing = narrowing_matrix.T
    pre, query, send, projection = pl.pallas_call(
        local_kernel,
        grid=(1,),
        out_shape=outs,
        in_specs=[pl.BlockSpec((RIM, value.shape[1]), lambda i: (0, 0)) for value in head_rows]
        + [VMEM]
        + [whole(value) for value in taps]
        + [VMEM] * len(kept)
        + [whole(widening_matrix), whole(narrowing), SMEM, HBM],
        out_specs=[VMEM] * 4,
        scratch_shapes=[pltpu.VMEM((2 * RIM, n), f32) for n in (WIDTH, STATE, STATE)]
        + [pltpu.SemaphoreType.DMA(())],
        interpret=INTERPRET,
        compiler_params=pltpu.CompilerParams(vmem_limit_bytes=56 << 20),
    )(*head_rows, near(rim), *taps, *kept, widening_matrix, narrowing, skip_path_factor, blend_result_matrix)
    rows = near(exchange(send, "y"))
    parts, send = call(
        row_kernel,
        [jax.ShapeDtypeStruct((ny, shard, STATE), bf16), shape((nzl, PAIR + TAIL, STATE), bf16)],
        [VMEM],
        compiler_params=ROOM,
    )(rows)
    weights = lax.all_gather(parts.reshape(ny * shard, STATE), ("c", "zh", "zl"), axis=0, tiled=True)
    weights = weights.reshape(-1, nzh * nzl, ny, shard // depth, depth, STATE)
    got = near(exchange(send, "zl"))
    send, state, logs = call(
        near_kernel,
        [shape((nzh, PAIR + TAIL, STATE), bf16), shape((PAIR, STATE), f32), shape((2, STATE), f32)],
        [VMEM],
        compiler_params=ROOM,
    )(got)
    got = near(exchange(send, "zh"))
    before = call(far_kernel, shape((ny, PAIR, STATE), bf16), [VMEM] * 4, compiler_params=ROOM)(
        got, near(state), near(logs), rows
    )
    incoming = exchange(before, "y")
    mixed = call(
        gate_kernel,
        shape((ntp, own_count, width), bf16),
        [VMEM] * 7,
        compiler_params=ROOM,
    )(
        near(pre),
        query,
        cum,
        near(incoming),
        multiplier_signal,
        cluster_scaling_vector.reshape(1, -1),
        near(projection),
    )
    mixed = exchange(mixed, TP)
    own, copies = call(
        norm_kernel,
        [shape((own_count, width), bf16), shape((nrows, own_count, width), bf16)],
        [VMEM] * 3,
    )(near(mixed), skip_stream_entering, feature_blend_scaling.reshape(1, -1))
    rows = exchange(copies, ROWS)
    out = call(
        mlp_kernel,
        shape((nrows, own_count, width), bf16),
        [VMEM, HBM],
        [pltpu.VMEM(weights.shape, bf16), pltpu.SemaphoreType.DMA((weights.shape[0], 4))],
    )(near(rows), weights)
    out = exchange(out, ROWS)
    return call(final_kernel, jax.ShapeDtypeStruct((own_count, width), bf16), [VMEM] * 2)(near(out), near(own))


def solution(mesh):
    torus = Mesh(mesh.devices.reshape(4, 4, 4, 4, 2), SP + TP)
    placed = (
        P(SP + TP, None),
        P(SP, TP),
        P(SP, TP),
        P(SP, TP),
        P(SP, TP),
        P(TP, SP),
        P(TP, SP),
        P(TP),
        P(None, TP),
        P(None, TP),
        P(None, TP),
        P(TP),
        P(TP),
        P(TP, None),
        P(),
        P(SP, TP),
        P(TP, SP),
    )
    return jax.shard_map(layer, mesh=torus, in_specs=placed, out_specs=P(SP + TP, None), check_vma=False)
```

```python
import jax
import jax.numpy as jnp
from jax import lax
from jax.experimental import pallas as pl
from jax.experimental.pallas import tpu as pltpu
from jax.sharding import Mesh
from jax.sharding import PartitionSpec as P

HEADS = 8
HEAD_DIM = 64
STATE = 128
BLOCK = 128
WIDTH = HEADS * HEAD_DIM
RIM = 8
PAIR = 2 * HEAD_DIM
TAIL = 16
SP = ("zh", "zl", "y")
TP = ("x", "c")
ROWS = ("y", "x")
EPSILON = 1e-05
INTERPRET = False
ROOM = pltpu.CompilerParams(vmem_limit_bytes=16 << 20)

f32 = jnp.float32
bf16 = jnp.bfloat16
VMEM = pl.BlockSpec(memory_space=pltpu.VMEM)
SMEM = pl.BlockSpec(memory_space=pltpu.SMEM)
HBM = pl.BlockSpec(memory_space=pl.ANY)


def call(kernel, outs, in_specs, scratch=(), **kw):
    single = not isinstance(outs, (list, tuple))
    return pl.pallas_call(
        kernel,
        out_shape=outs,
        in_specs=in_specs,
        out_specs=VMEM if single else [VMEM] * len(outs),
        scratch_shapes=list(scratch),
        interpret=INTERPRET,
        **kw,
    )


def shape(dims, kind):
    return jax.ShapeDtypeStruct(dims, kind) if INTERPRET else pltpu.VMEM(dims, kind)


def near(value):
    return value if INTERPRET else pltpu.with_memory_space_constraint(value, pltpu.VMEM)


def exchange(value, axes):
    return lax.all_to_all(value, axes, split_axis=0, concat_axis=0, tiled=True)


def dot(a, b, dims, **kw):
    return lax.dot_general(a, b, (dims, ((), ())), preferred_element_type=f32, **kw)


def spread(rows, width):
    head = lax.broadcasted_iota(jnp.int32, (HEADS, HEADS * width), 0)
    lane = lax.broadcasted_iota(jnp.int32, (HEADS, HEADS * width), 1)
    chosen = jnp.where(lane // width == head, 1.0, 0.0).astype(f32)
    return dot(rows, chosen, ((0,), (0,)), precision=lax.Precision.HIGHEST)


def silu(value):
    return value / (1.0 + jnp.exp(-value))


def convolve(room, taps_ref, count):
    taps = taps_ref[...].astype(f32)
    width = taps.shape[0]
    total = None
    for k in range(width):
        start = RIM - width + 1 + k
        term = room[start : start + count, :] * taps[k : k + 1, :]
        total = term if total is None else total + term
    return total


def put_state(ref, place, start, state, logs):
    ref[place, start : start + PAIR, :] = state.astype(bf16)
    row = lax.broadcasted_iota(jnp.int32, (TAIL, STATE), 0)
    tail = jnp.zeros((TAIL, STATE), f32)
    for h in range(2):
        whole = jnp.broadcast_to(logs[h : h + 1, :], (TAIL, STATE))
        high = whole.astype(bf16).astype(f32)
        tail = jnp.where(row == 2 * h, high, jnp.where(row == 2 * h + 1, whole - high, tail))
    ref[place, start + PAIR : start + PAIR + TAIL, :] = tail.astype(bf16)


def take_state(ref, place, start):
    state = ref[place, start : start + PAIR, :].astype(f32)
    tail = ref[place, start + PAIR : start + PAIR + TAIL, :].astype(f32)
    return state, jnp.concatenate([tail[2 * h : 2 * h + 1, :] + tail[2 * h + 1 : 2 * h + 2, :] for h in range(2)], axis=0)


def factor(logs):
    grown = jnp.exp(logs)
    return jnp.concatenate([jnp.broadcast_to(grown[h : h + 1, :], (HEAD_DIM, STATE)) for h in range(2)], axis=0)


def first_kernel(x_ref, b_ref, c_ref, rim_ref):
    rim_ref[:, 0:WIDTH] = x_ref[...]
    rim_ref[:, WIDTH : WIDTH + STATE] = b_ref[...]
    rim_ref[:, WIDTH + STATE : WIDTH + 2 * STATE] = c_ref[...]


def early_kernel(
    x_ref, b_ref, c_ref, xt_ref, bt_ref, ct_ref, dt_ref, shrink_ref, speed_ref, w_ref,
    x_out, b_out, c_out, cum_ref, weight_ref, mask_ref, w_out, x_room, b_room, c_room, sem,
):
    copy = pltpu.make_async_copy(w_ref.at[0 : w_out.shape[0]], w_out, sem)
    copy.start()
    for src_ref, taps_ref, out_ref, room in (
        (x_ref, xt_ref, x_out, x_room), (b_ref, bt_ref, b_out, b_room), (c_ref, ct_ref, c_out, c_room)
    ):
        room[0:RIM, :] = jnp.zeros((RIM, room.shape[1]), f32)
        room[RIM : RIM + BLOCK, :] = src_ref[...].astype(f32)
        out_ref[...] = convolve(room, taps_ref, BLOCK)
    before = dt_ref[...]
    steps = jnp.maximum(before, 0.0) + jnp.log1p(jnp.exp(-jnp.abs(before)))
    head = lax.broadcasted_iota(jnp.int32, (HEADS, BLOCK), 0)
    token = lax.broadcasted_iota(jnp.int32, (HEADS, BLOCK), 1)
    speed = jnp.zeros((HEADS, BLOCK), f32)
    for h in range(HEADS):
        speed = jnp.where(head == h, speed_ref[h], speed)
    cum = shrink_ref[...] - jnp.exp(speed) * steps
    reach = 1
    while reach < BLOCK:
        cum = cum + jnp.where(token >= reach, pltpu.roll(cum, reach, 1), 0.0)
        reach *= 2
    cum_ref[...] = cum
    weight_ref[...] = spread(steps * jnp.exp(cum[:, BLOCK - 1 : BLOCK] - cum), HEAD_DIM)
    columns = spread(cum, BLOCK)
    later = lax.broadcasted_iota(jnp.int32, (BLOCK, BLOCK), 0)
    earlier = lax.broadcasted_iota(jnp.int32, (BLOCK, BLOCK), 1)
    causal = later >= earlier
    for h in range(HEADS):
        away = columns[:, h * BLOCK : (h + 1) * BLOCK] - cum[h : h + 1, :]
        mask_ref[h] = jnp.exp(jnp.where(causal, away, -jnp.inf)) * steps[h : h + 1, :]
    copy.wait()


def local_kernel(
    x_ref, b_ref, c_ref, rim_ref, xt_ref, bt_ref, ct_ref, x_sum, b_sum, c_sum, cum_ref, weight_ref, mask_ref,
    up_ref, down_ref, skip_ref, w_ref,
    pre_ref, query_ref, send_ref, w_out, x_room, b_room, c_room, sem,
):
    half = w_out.shape[0]
    copy = pltpu.make_async_copy(w_ref.at[half : 2 * half], w_out, sem)
    copy.start()
    rows = []
    lane = 0
    for src_ref, taps_ref, sum_ref, room in (
        (x_ref, xt_ref, x_sum, x_room), (b_ref, bt_ref, b_sum, b_room), (c_ref, ct_ref, c_sum, c_room)
    ):
        room[0:RIM, :] = rim_ref[:, lane : lane + room.shape[1]].astype(f32)
        room[RIM : 2 * RIM, :] = src_ref[...].astype(f32)
        lane += room.shape[1]
        head = convolve(room, taps_ref, RIM)
        rows.append(silu(jnp.concatenate([head, sum_ref[RIM:BLOCK, :]], axis=0)))
    values, keys, query = rows[0], rows[1].astype(bf16), rows[2].astype(bf16)
    query_ref[...] = query
    last = cum_ref[:, BLOCK - 1 : BLOCK]
    state = dot((values * weight_ref[...]).astype(bf16), keys, ((0,), (0,)))
    pieces = send_ref.shape[0]
    depth, units = up_ref.shape
    slabs = units // pieces // STATE
    for k in range(pieces):
        for j in range(slabs):
            lanes = slice((k * slabs + j) * STATE, (k * slabs + j + 1) * STATE)
            send_ref[k, j * depth : (j + 1) * depth, :] = up_ref[:, lanes]
            send_ref[k, (slabs + j) * depth : (slabs + j + 1) * depth, :] = down_ref[:, lanes]
        put_state(send_ref, k, 2 * slabs * depth, state[k * PAIR : (k + 1) * PAIR, :], last[2 * k : 2 * k + 2, :])
    scores = dot(query, keys, ((1,), (1,)))
    first = lax.broadcasted_iota(jnp.int32, (BLOCK, 2 * HEAD_DIM), 1) < HEAD_DIM
    for pair in range(HEADS // 2):
        lanes = slice(pair * 2 * HEAD_DIM, (pair + 1) * 2 * HEAD_DIM)
        two = values[:, lanes]
        two_low = two.astype(bf16)
        parts = []
        for h in (2 * pair, 2 * pair + 1):
            mixing = scores * mask_ref[h]
            parts.append(dot(mixing.astype(bf16), two_low, ((1,), (0,))))
        within = jnp.where(first, parts[0], parts[1])
        skip = jnp.where(first, skip_ref[2 * pair], skip_ref[2 * pair + 1])
        pre_ref[:, lanes] = within + skip * two
    copy.wait()


def row_kernel(got_ref, shard_ref, send_ref):
    start = shard_ref.shape[1]
    state = logs = None
    for k in range(got_ref.shape[0]):
        shard_ref[k] = got_ref[k, 0:start, :]
        more, step = take_state(got_ref, k, start)
        state, logs = (more, step) if state is None else (state * factor(step) + more, logs + step)
    for k in range(send_ref.shape[0]):
        put_state(send_ref, k, 0, state, logs)


def near_kernel(got_ref, send_ref, state_ref, logs_ref):
    here = lax.axis_index("zl")
    state = before = jnp.zeros((PAIR, STATE), f32)
    logs = passed = jnp.zeros((2, STATE), f32)
    for k in range(got_ref.shape[0]):
        more, step = take_state(got_ref, k, 0)
        state, logs = state * factor(step) + more, logs + step
        before, passed = jnp.where(k < here, state, before), jnp.where(k < here, logs, passed)
    state_ref[...] = before
    logs_ref[...] = passed
    for k in range(send_ref.shape[0]):
        put_state(send_ref, k, 0, state, logs)


def far_kernel(got_ref, state_ref, logs_ref, rows_ref, out_ref):
    here = lax.axis_index("zh")
    state = before = jnp.zeros((PAIR, STATE), f32)
    for k in range(got_ref.shape[0] - 1):
        more, step = take_state(got_ref, k, 0)
        state = state * factor(step) + more
        before = jnp.where(k < here, state, before)
    state = before * factor(logs_ref[...]) + state_ref[...]
    start = rows_ref.shape[1] - PAIR - TAIL
    for k in range(rows_ref.shape[0]):
        out_ref[k] = state.astype(bf16)
        if k + 1 < rows_ref.shape[0]:
            more, step = take_state(rows_ref, k, start)
            state = state * factor(step) + more


def gate_kernel(pre_ref, query_ref, cum_ref, inc_ref, gate_ref, gain_ref, upper_ref, lower_ref, out_ref):
    inc = inc_ref[...].reshape(WIDTH, STATE)
    arriving = dot(query_ref[...], inc, ((1,), (1,))) * spread(jnp.exp(cum_ref[...]), HEAD_DIM)
    gated = (pre_ref[...] + arriving) * silu(gate_ref[...].astype(f32))
    scale = lax.rsqrt(jnp.mean(gated * gated, axis=-1, keepdims=True) + EPSILON)
    heads_out = (gated * scale * gain_ref[...]).astype(bf16)
    half = upper_ref.shape[0]
    out = dot(heads_out[:, 0:half], upper_ref[...], ((1,), (0,)))
    out = out + dot(heads_out[:, half : 2 * half], lower_ref[...], ((1,), (0,)))
    out_ref[...] = out.astype(bf16).reshape(out_ref.shape)


def norm_kernel(got_ref, skip_ref, gain_ref, own_ref, copies_ref):
    total = got_ref[0].astype(f32)
    for k in range(1, got_ref.shape[0]):
        total = total + got_ref[k].astype(f32)
    total = total.reshape(own_ref.shape)
    own = (skip_ref[...].astype(f32) + total.astype(bf16).astype(f32)).astype(bf16)
    own_ref[...] = own
    wide = own.astype(f32)
    scale = lax.rsqrt(jnp.mean(wide * wide, axis=-1, keepdims=True) + EPSILON)
    normed = (wide * scale * gain_ref[...]).astype(bf16)
    for k in range(copies_ref.shape[0]):
        copies_ref[k] = normed.reshape(copies_ref.shape[1:])


def mlp_kernel(rows_ref, w_ref, out_ref, w_room, sems):
    halves, shards, inner, slabs, each_depth, lanes = w_ref.shape
    pieces = sems.shape[2]
    take = shards // pieces
    size = take * inner * each_depth
    copies = []
    for part in range(2):
        some = pl.ds(part * (slabs // 2), slabs // 2)
        for j in range(pieces):
            for k in range(halves):
                place = (k, pl.ds(j * take, take), slice(None), some)
                copy = pltpu.make_async_copy(w_ref.at[place], w_room.at[place], sems.at[part, k, j])
                copy.start()
                copies.append(copy)

    def piece(k, j, first):
        parts = [w_room[k, j * take : (j + 1) * take, :, n, :, :] for n in (first, first + 1)]
        return jnp.concatenate([p.reshape(size, lanes) for p in parts], axis=1)

    depth = rows_ref.shape[-1]
    rows = rows_ref[...].reshape(-1, depth)
    lifted = [None] * halves
    for j in range(pieces):
        for k in range(halves):
            copies[j * halves + k].wait()
            part = dot(rows[:, j * size : (j + 1) * size], piece(k, j, 0), ((1,), (0,)))
            lifted[k] = part if lifted[k] is None else lifted[k] + part
    hidden = []
    for k in range(halves):
        up = jnp.maximum(lifted[k], 0.0)
        hidden.append((up * up).astype(bf16))
    for j in range(pieces):
        total = None
        for k in range(halves):
            copies[(pieces + j) * halves + k].wait()
            part = dot(hidden[k], piece(k, j, slabs // 2), ((1,), (1,)))
            total = part if total is None else total + part
        out_ref[:, :, :, j * size : (j + 1) * size] = total.astype(bf16).reshape(*out_ref.shape[:3], size)


def final_kernel(got_ref, own_ref, out_ref):
    total = got_ref[0].astype(f32)
    for k in range(1, got_ref.shape[0]):
        total = total + got_ref[k].astype(f32)
    total = total.reshape(own_ref.shape)
    out_ref[...] = (own_ref[...].astype(f32) + total.astype(bf16).astype(f32)).astype(bf16)


def layer(
    skip_stream_entering,
    content_signal_matrix,
    writer_signal_matrix,
    reader_signal_matrix,
    multiplier_signal,
    interval_before_softplus,
    extra_log_shrink,
    log_forget_speed,
    content_filter_coefs,
    writer_filter_coefs,
    reader_filter_coefs,
    skip_path_factor,
    cluster_scaling_vector,
    blend_result_matrix,
    feature_blend_scaling,
    widening_matrix,
    narrowing_matrix,
):
    ny, nzl, nzh = (lax.axis_size(name) for name in ("y", "zl", "zh"))
    nsp = nzh * nzl * ny
    ntp = lax.axis_size("x") * lax.axis_size("c")
    nrows = ny * lax.axis_size("x")
    own_count, width = skip_stream_entering.shape
    own_tiles = (own_count // 8, 8, width)
    depth, units = widening_matrix.shape
    shard = 2 * depth * units // ny // STATE

    rim = pl.pallas_call(
        first_kernel,
        grid=(1,),
        out_shape=shape((RIM, WIDTH + 2 * STATE), bf16),
        in_specs=[pl.BlockSpec((RIM, n), lambda i: (BLOCK // RIM - 1, 0)) for n in (WIDTH, STATE, STATE)],
        out_specs=pl.BlockSpec((RIM, WIDTH + 2 * STATE), lambda i: (0, 0)),
        interpret=INTERPRET,
    )(content_signal_matrix, writer_signal_matrix, reader_signal_matrix)
    rim = lax.ppermute(rim, SP, [(k, k + 1) for k in range(nsp - 1)])
    half = (blend_result_matrix.shape[0] // 2, width)
    *sums, cum, weight, mask, upper = call(
        early_kernel,
        [
            shape((BLOCK, WIDTH), f32),
            shape((BLOCK, STATE), f32),
            shape((BLOCK, STATE), f32),
            shape((HEADS, BLOCK), f32),
            shape((BLOCK, WIDTH), f32),
            shape((HEADS, BLOCK, BLOCK), f32),
            shape(half, bf16),
        ],
        [VMEM] * 8 + [SMEM, HBM],
        [pltpu.VMEM((RIM + BLOCK, n), f32) for n in (WIDTH, STATE, STATE)] + [pltpu.SemaphoreType.DMA(())],
        compiler_params=pltpu.CompilerParams(vmem_limit_bytes=56 << 20),
    )(
        content_signal_matrix,
        writer_signal_matrix,
        reader_signal_matrix,
        content_filter_coefs,
        writer_filter_coefs,
        reader_filter_coefs,
        interval_before_softplus,
        extra_log_shrink,
        log_forget_speed,
        blend_result_matrix,
    )

    def whole(value):
        zeros = (0,) * value.ndim
        return pl.BlockSpec(value.shape, lambda i: zeros)

    head_rows = (content_signal_matrix, writer_signal_matrix, reader_signal_matrix)
    taps = (content_filter_coefs, writer_filter_coefs, reader_filter_coefs)
    kept = [near(value) for value in (*sums, cum, weight, mask)]
    outs = [
        shape((BLOCK, WIDTH), f32),
        shape((BLOCK, STATE), bf16),
        shape((ny, shard + PAIR + TAIL, STATE), bf16),
        shape(half, bf16),
    ]
    narrowing = narrowing_matrix.T
    pre, query, send, lower = pl.pallas_call(
        local_kernel,
        grid=(1,),
        out_shape=outs,
        in_specs=[pl.BlockSpec((RIM, value.shape[1]), lambda i: (0, 0)) for value in head_rows]
        + [VMEM]
        + [whole(value) for value in taps]
        + [VMEM] * len(kept)
        + [whole(widening_matrix), whole(narrowing), SMEM, HBM],
        out_specs=[VMEM] * 4,
        scratch_shapes=[pltpu.VMEM((2 * RIM, n), f32) for n in (WIDTH, STATE, STATE)]
        + [pltpu.SemaphoreType.DMA(())],
        interpret=INTERPRET,
        compiler_params=pltpu.CompilerParams(vmem_limit_bytes=56 << 20),
    )(*head_rows, near(rim), *taps, *kept, widening_matrix, narrowing, skip_path_factor, blend_result_matrix)
    rows = near(exchange(send, "y"))
    parts, send = call(
        row_kernel,
        [jax.ShapeDtypeStruct((ny, shard, STATE), bf16), shape((nzl, PAIR + TAIL, STATE), bf16)],
        [VMEM],
        compiler_params=ROOM,
    )(rows)
    weights = lax.all_gather(parts.reshape(ny * shard, STATE), ("c", "zh", "zl"), axis=0, tiled=True)
    weights = weights.reshape(-1, nzh * nzl, ny, shard // depth, depth, STATE)
    got = near(exchange(send, "zl"))
    send, state, logs = call(
        near_kernel,
        [shape((nzh, PAIR + TAIL, STATE), bf16), shape((PAIR, STATE), f32), shape((2, STATE), f32)],
        [VMEM],
        compiler_params=ROOM,
    )(got)
    got = near(exchange(send, "zh"))
    before = call(far_kernel, shape((ny, PAIR, STATE), bf16), [VMEM] * 4, compiler_params=ROOM)(
        got, near(state), near(logs), rows
    )
    incoming = exchange(before, "y")
    mixed = call(
        gate_kernel,
        shape((ntp, *own_tiles), bf16),
        [VMEM] * 8,
        compiler_params=ROOM,
    )(
        near(pre),
        near(query),
        near(cum),
        near(incoming),
        multiplier_signal,
        cluster_scaling_vector.reshape(1, -1),
        near(upper),
        near(lower),
    )
    mixed = exchange(mixed, TP)
    own, copies = call(
        norm_kernel,
        [shape((own_count, width), bf16), shape((nrows, *own_tiles), bf16)],
        [VMEM] * 3,
    )(near(mixed), skip_stream_entering, feature_blend_scaling.reshape(1, -1))
    rows = exchange(copies, ROWS)
    out = call(
        mlp_kernel,
        shape((nrows, *own_tiles), bf16),
        [VMEM, HBM],
        [pltpu.VMEM(weights.shape, bf16), pltpu.SemaphoreType.DMA((2, weights.shape[0], 4))],
    )(near(rows), weights)
    out = exchange(out, ROWS)
    return call(final_kernel, jax.ShapeDtypeStruct((own_count, width), bf16), [VMEM] * 2)(near(out), near(own))


def solution(mesh):
    torus = Mesh(mesh.devices.reshape(4, 4, 4, 4, 2), SP + TP)
    placed = (
        P(SP + TP, None),
        P(SP, TP),
        P(SP, TP),
        P(SP, TP),
        P(SP, TP),
        P(TP, SP),
        P(TP, SP),
        P(TP),
        P(None, TP),
        P(None, TP),
        P(None, TP),
        P(TP),
        P(TP),
        P(TP, None),
        P(),
        P(SP, TP),
        P(TP, SP),
    )
    return jax.shard_map(layer, mesh=torus, in_specs=placed, out_specs=P(SP + TP, None), check_vma=False)
```

```python
import functools

import jax
import jax.numpy as jnp
from jax import lax
from jax.experimental import pallas as pl
from jax.experimental.pallas import tpu as pltpu
from jax.sharding import Mesh
from jax.sharding import PartitionSpec as P

HEADS = 8
HEAD_DIM = 64
STATE = 128
BLOCK = 128
WIDTH = HEADS * HEAD_DIM
RIM = 8
TAIL = 16
NEAR = ("zl", "y")
SP = ("zh", "zl", "y")
TP = ("x", "c")
ROWS = ("y", "x")
EPSILON = 1e-05
INTERPRET = False
ROOM = pltpu.CompilerParams(vmem_limit_bytes=16 << 20)

f32 = jnp.float32
bf16 = jnp.bfloat16
VMEM = pl.BlockSpec(memory_space=pltpu.VMEM)
SMEM = pl.BlockSpec(memory_space=pltpu.SMEM)
HBM = pl.BlockSpec(memory_space=pl.ANY)


def call(kernel, outs, in_specs, scratch=(), **kw):
    single = not isinstance(outs, (list, tuple))
    return pl.pallas_call(
        kernel,
        out_shape=outs,
        in_specs=in_specs,
        out_specs=VMEM if single else [VMEM] * len(outs),
        scratch_shapes=list(scratch),
        interpret=INTERPRET,
        **kw,
    )


def shape(dims, kind):
    return jax.ShapeDtypeStruct(dims, kind) if INTERPRET else pltpu.VMEM(dims, kind)


def near(value):
    return value if INTERPRET else pltpu.with_memory_space_constraint(value, pltpu.VMEM)


def exchange(value, axes):
    return lax.all_to_all(value, axes, split_axis=0, concat_axis=0, tiled=True)


def dot(a, b, dims, **kw):
    return lax.dot_general(a, b, (dims, ((), ())), preferred_element_type=f32, **kw)


def spread(rows, width):
    head = lax.broadcasted_iota(jnp.int32, (HEADS, HEADS * width), 0)
    lane = lax.broadcasted_iota(jnp.int32, (HEADS, HEADS * width), 1)
    chosen = jnp.where(lane // width == head, 1.0, 0.0).astype(f32)
    return dot(rows, chosen, ((0,), (0,)), precision=lax.Precision.HIGHEST)


def silu(value):
    return value / (1.0 + jnp.exp(-value))


def convolve(room, taps_ref, count):
    taps = taps_ref[...].astype(f32)
    width = taps.shape[0]
    total = None
    for k in range(width):
        start = RIM - width + 1 + k
        term = room[start : start + count, :] * taps[k : k + 1, :]
        total = term if total is None else total + term
    return total


def put_state(ref, place, start, state, log):
    count = state.shape[0]
    ref[place, start : start + count, :] = state.astype(bf16)
    row = lax.broadcasted_iota(jnp.int32, (TAIL, STATE), 0)
    whole = jnp.broadcast_to(log, (TAIL, STATE))
    high = whole.astype(bf16).astype(f32)
    tail = jnp.where(row == 0, high, jnp.where(row == 1, whole - high, 0.0))
    ref[place, start + count : start + count + TAIL, :] = tail.astype(bf16)


def take_state(ref, place, start):
    end = ref.shape[1] - TAIL
    tail = ref[place, end : end + TAIL, :].astype(f32)
    return ref[place, start:end, :].astype(f32), tail[0:1, :] + tail[1:2, :]


def first_kernel(x_ref, b_ref, c_ref, rim_ref):
    rim_ref[:, 0:WIDTH] = x_ref[...]
    rim_ref[:, WIDTH : WIDTH + STATE] = b_ref[...]
    rim_ref[:, WIDTH + STATE : WIDTH + 2 * STATE] = c_ref[...]


def early_kernel(
    x_ref, b_ref, c_ref, xt_ref, bt_ref, ct_ref, dt_ref, shrink_ref, speed_ref,
    x_out, b_out, c_out, cum_ref, weight_ref, mask_ref, x_room, b_room, c_room,
):
    for src_ref, taps_ref, out_ref, room in (
        (x_ref, xt_ref, x_out, x_room), (b_ref, bt_ref, b_out, b_room), (c_ref, ct_ref, c_out, c_room)
    ):
        room[0:RIM, :] = jnp.zeros((RIM, room.shape[1]), f32)
        room[RIM : RIM + BLOCK, :] = src_ref[...].astype(f32)
        out_ref[...] = convolve(room, taps_ref, BLOCK)
    before = dt_ref[...]
    steps = jnp.maximum(before, 0.0) + jnp.log1p(jnp.exp(-jnp.abs(before)))
    head = lax.broadcasted_iota(jnp.int32, (HEADS, BLOCK), 0)
    token = lax.broadcasted_iota(jnp.int32, (HEADS, BLOCK), 1)
    speed = jnp.zeros((HEADS, BLOCK), f32)
    for h in range(HEADS):
        speed = jnp.where(head == h, speed_ref[h], speed)
    cum = shrink_ref[...] - jnp.exp(speed) * steps
    reach = 1
    while reach < BLOCK:
        cum = cum + jnp.where(token >= reach, pltpu.roll(cum, reach, 1), 0.0)
        reach *= 2
    cum_ref[...] = cum
    weight_ref[...] = spread(steps * jnp.exp(cum[:, BLOCK - 1 : BLOCK] - cum), HEAD_DIM)
    columns = spread(cum, BLOCK)
    later = lax.broadcasted_iota(jnp.int32, (BLOCK, BLOCK), 0)
    earlier = lax.broadcasted_iota(jnp.int32, (BLOCK, BLOCK), 1)
    causal = later >= earlier
    for h in range(HEADS):
        away = columns[:, h * BLOCK : (h + 1) * BLOCK] - cum[h : h + 1, :]
        mask_ref[h] = jnp.exp(jnp.where(causal, away, -jnp.inf)) * steps[h : h + 1, :]


def local_kernel(
    slices, x_ref, b_ref, c_ref, rim_ref, xt_ref, bt_ref, ct_ref, x_sum, b_sum, c_sum, cum_ref, weight_ref, mask_ref,
    up_ref, down_ref, skip_ref,
    pre_ref, query_ref, send_ref, x_room, b_room, c_room,
):
    rows = []
    lane = 0
    for src_ref, taps_ref, sum_ref, room in (
        (x_ref, xt_ref, x_sum, x_room), (b_ref, bt_ref, b_sum, b_room), (c_ref, ct_ref, c_sum, c_room)
    ):
        room[0:RIM, :] = rim_ref[:, lane : lane + room.shape[1]].astype(f32)
        room[RIM : 2 * RIM, :] = src_ref[...].astype(f32)
        lane += room.shape[1]
        head = convolve(room, taps_ref, RIM)
        rows.append(silu(jnp.concatenate([head, sum_ref[RIM:BLOCK, :]], axis=0)))
    values, keys, query = rows[0], rows[1].astype(bf16), rows[2].astype(bf16)
    query_ref[...] = query
    last = cum_ref[:, BLOCK - 1 : BLOCK]
    state = dot((values * weight_ref[...]).astype(bf16), keys, ((0,), (0,)))
    pieces = send_ref.shape[0]
    depth, units = up_ref.shape
    count = WIDTH // pieces
    slabs = units // slices // STATE
    for place in range(pieces):
        slab, k = divmod(place, slices)
        source = up_ref if slab < slabs else down_ref
        first_lane = (k * slabs + slab % slabs) * STATE
        send_ref[place, 0:depth, :] = source[:, first_lane : first_lane + STATE]
        h = place * count // HEAD_DIM
        put_state(send_ref, place, depth, state[place * count : (place + 1) * count, :], last[h : h + 1, :])
    scores = dot(query, keys, ((1,), (1,)))
    first = lax.broadcasted_iota(jnp.int32, (BLOCK, 2 * HEAD_DIM), 1) < HEAD_DIM
    for pair in range(HEADS // 2):
        lanes = slice(pair * 2 * HEAD_DIM, (pair + 1) * 2 * HEAD_DIM)
        two = values[:, lanes]
        two_low = two.astype(bf16)
        parts = []
        for h in (2 * pair, 2 * pair + 1):
            mixing = scores * mask_ref[h]
            parts.append(dot(mixing.astype(bf16), two_low, ((1,), (0,))))
        within = jnp.where(first, parts[0], parts[1])
        skip = jnp.where(first, skip_ref[2 * pair], skip_ref[2 * pair + 1])
        pre_ref[:, lanes] = within + skip * two


def near_kernel(got_ref, shard_ref, send_ref):
    start = shard_ref.shape[1]
    shard_ref[...] = got_ref[:, 0:start, :]
    state = log = None
    for k in range(got_ref.shape[0]):
        more, step = take_state(got_ref, k, start)
        state, log = (more, step) if state is None else (state * jnp.exp(step) + more, log + step)
    for k in range(send_ref.shape[0]):
        put_state(send_ref, k, 0, state, log)


def far_kernel(got_ref, near_ref, out_ref):
    here = lax.axis_index("zh")
    count = out_ref.shape[1]
    state = before = jnp.zeros((count, STATE), f32)
    for k in range(got_ref.shape[0] - 1):
        more, step = take_state(got_ref, k, 0)
        state = state * jnp.exp(step) + more
        before = jnp.where(k < here, state, before)
    state = before
    start = near_ref.shape[1] - count - TAIL
    for k in range(near_ref.shape[0]):
        out_ref[k] = state.astype(bf16)
        if k + 1 < near_ref.shape[0]:
            more, step = take_state(near_ref, k, start)
            state = state * jnp.exp(step) + more


def gate_kernel(pre_ref, query_ref, cum_ref, inc_ref, gate_ref, gain_ref, w_ref, out_ref):
    inc = inc_ref[...].reshape(WIDTH, STATE)
    arriving = dot(query_ref[...], inc, ((1,), (1,))) * spread(jnp.exp(cum_ref[...]), HEAD_DIM)
    gated = (pre_ref[...] + arriving) * silu(gate_ref[...].astype(f32))
    scale = lax.rsqrt(jnp.mean(gated * gated, axis=-1, keepdims=True) + EPSILON)
    heads_out = (gated * scale * gain_ref[...]).astype(bf16)
    out = dot(heads_out, w_ref[...], ((1,), (0,)))
    out_ref[...] = out.astype(bf16).reshape(out_ref.shape)


def norm_kernel(got_ref, skip_ref, gain_ref, own_ref, copies_ref):
    total = got_ref[0].astype(f32)
    for k in range(1, got_ref.shape[0]):
        total = total + got_ref[k].astype(f32)
    total = total.reshape(own_ref.shape)
    own = (skip_ref[...].astype(f32) + total.astype(bf16).astype(f32)).astype(bf16)
    own_ref[...] = own
    wide = own.astype(f32)
    scale = lax.rsqrt(jnp.mean(wide * wide, axis=-1, keepdims=True) + EPSILON)
    normed = (wide * scale * gain_ref[...]).astype(bf16)
    for k in range(copies_ref.shape[0]):
        copies_ref[k] = normed.reshape(copies_ref.shape[1:])


def mlp_kernel(rows_ref, w_ref, out_ref, w_room, sems):
    halves, pieces, slabs, size, _ = w_ref.shape
    copies = []
    for part in range(2):
        some = pl.ds(part * (slabs // 2), slabs // 2)
        for j in range(pieces):
            for k in range(halves):
                copy = pltpu.make_async_copy(w_ref.at[k, j, some], w_room.at[k, j, some], sems.at[part, k, j])
                copy.start()
                copies.append(copy)

    def piece(k, j, first):
        return jnp.concatenate([w_room[k, j, n] for n in range(first, first + slabs // 2)], axis=1)

    depth = rows_ref.shape[-1]
    rows = rows_ref[...].reshape(-1, depth)
    lifted = [None] * halves
    for j in range(pieces):
        for k in range(halves):
            copies[j * halves + k].wait()
            part = dot(rows[:, j * size : (j + 1) * size], piece(k, j, 0), ((1,), (0,)))
            lifted[k] = part if lifted[k] is None else lifted[k] + part
    hidden = []
    for k in range(halves):
        up = jnp.maximum(lifted[k], 0.0)
        hidden.append((up * up).astype(bf16))
    for j in range(pieces):
        total = None
        for k in range(halves):
            copies[(pieces + j) * halves + k].wait()
            part = dot(hidden[k], piece(k, j, slabs // 2), ((1,), (1,)))
            total = part if total is None else total + part
        out_ref[:, :, :, j * size : (j + 1) * size] = total.astype(bf16).reshape(*out_ref.shape[:3], size)


def final_kernel(got_ref, own_ref, out_ref):
    total = got_ref[0].astype(f32)
    for k in range(1, got_ref.shape[0]):
        total = total + got_ref[k].astype(f32)
    total = total.reshape(own_ref.shape)
    out_ref[...] = (own_ref[...].astype(f32) + total.astype(bf16).astype(f32)).astype(bf16)


def layer(
    skip_stream_entering,
    content_signal_matrix,
    writer_signal_matrix,
    reader_signal_matrix,
    multiplier_signal,
    interval_before_softplus,
    extra_log_shrink,
    log_forget_speed,
    content_filter_coefs,
    writer_filter_coefs,
    reader_filter_coefs,
    skip_path_factor,
    cluster_scaling_vector,
    blend_result_matrix,
    feature_blend_scaling,
    widening_matrix,
    narrowing_matrix,
):
    ny, nzl, nzh = (lax.axis_size(name) for name in ("y", "zl", "zh"))
    nsp = nzh * nzl * ny
    ntp = lax.axis_size("x") * lax.axis_size("c")
    nrows = ny * lax.axis_size("x")
    own_count, width = skip_stream_entering.shape
    own_tiles = (own_count // 8, 8, width)
    depth, _ = widening_matrix.shape
    pieces = nzl * ny
    count = WIDTH // pieces

    rim = pl.pallas_call(
        first_kernel,
        grid=(1,),
        out_shape=shape((RIM, WIDTH + 2 * STATE), bf16),
        in_specs=[pl.BlockSpec((RIM, n), lambda i: (BLOCK // RIM - 1, 0)) for n in (WIDTH, STATE, STATE)],
        out_specs=pl.BlockSpec((RIM, WIDTH + 2 * STATE), lambda i: (0, 0)),
        interpret=INTERPRET,
        compiler_params=pltpu.CompilerParams(vmem_limit_bytes=54 << 20),
    )(content_signal_matrix, writer_signal_matrix, reader_signal_matrix)
    rim = lax.ppermute(rim, SP, [(k, k + 1) for k in range(nsp - 1)])
    *sums, cum, weight, mask = call(
        early_kernel,
        [
            shape((BLOCK, WIDTH), f32),
            shape((BLOCK, STATE), f32),
            shape((BLOCK, STATE), f32),
            shape((HEADS, BLOCK), f32),
            shape((BLOCK, WIDTH), f32),
            shape((HEADS, BLOCK, BLOCK), f32),
        ],
        [VMEM] * 8 + [SMEM],
        [pltpu.VMEM((RIM + BLOCK, n), f32) for n in (WIDTH, STATE, STATE)],
        compiler_params=pltpu.CompilerParams(vmem_limit_bytes=54 << 20),
    )(
        content_signal_matrix,
        writer_signal_matrix,
        reader_signal_matrix,
        content_filter_coefs,
        writer_filter_coefs,
        reader_filter_coefs,
        interval_before_softplus,
        extra_log_shrink,
        log_forget_speed,
    )

    def whole(value):
        zeros = (0,) * value.ndim
        return pl.BlockSpec(value.shape, lambda i: zeros)

    head_rows = (content_signal_matrix, writer_signal_matrix, reader_signal_matrix)
    taps = (content_filter_coefs, writer_filter_coefs, reader_filter_coefs)
    kept = [near(value) for value in (*sums, cum, weight, mask)]
    outs = [
        shape((BLOCK, WIDTH), f32),
        shape((BLOCK, STATE), bf16),
        shape((pieces, depth + count + TAIL, STATE), bf16),
    ]
    narrowing = narrowing_matrix.T
    pre, query, send = pl.pallas_call(
        functools.partial(local_kernel, ny),
        grid=(1,),
        out_shape=outs,
        in_specs=[pl.BlockSpec((RIM, value.shape[1]), lambda i: (0, 0)) for value in head_rows]
        + [VMEM]
        + [whole(value) for value in taps]
        + [VMEM] * len(kept)
        + [whole(widening_matrix), whole(narrowing), SMEM],
        out_specs=[VMEM] * 3,
        scratch_shapes=[pltpu.VMEM((2 * RIM, n), f32) for n in (WIDTH, STATE, STATE)],
        interpret=INTERPRET,
        compiler_params=pltpu.CompilerParams(vmem_limit_bytes=54 << 20),
    )(*head_rows, near(rim), *taps, *kept, widening_matrix, narrowing, skip_path_factor)
    got = near(exchange(send, NEAR))
    parts, send = call(
        near_kernel,
        [jax.ShapeDtypeStruct((pieces, depth, STATE), bf16), shape((nzh, count + TAIL, STATE), bf16)],
        [VMEM],
        compiler_params=ROOM,
    )(got)
    weights = lax.all_gather(parts.reshape(pieces * depth, STATE), ("c", "zh", "zl"), axis=0, tiled=True)
    weights = weights.reshape(-1, nzh, nzl, pieces * depth, STATE)
    far = near(exchange(send, "zh"))
    before = call(far_kernel, shape((pieces, count, STATE), bf16), [VMEM] * 2, compiler_params=ROOM)(far, got)
    incoming = exchange(before, NEAR)
    mixed = call(
        gate_kernel,
        shape((ntp, *own_tiles), bf16),
        [VMEM] * 7,
        compiler_params=ROOM,
    )(
        near(pre),
        near(query),
        near(cum),
        near(incoming),
        near(multiplier_signal),
        near(cluster_scaling_vector.reshape(1, -1)),
        near(blend_result_matrix),
    )
    mixed = exchange(mixed, TP)
    own, copies = call(
        norm_kernel,
        [shape((own_count, width), bf16), shape((nrows, *own_tiles), bf16)],
        [VMEM] * 3,
    )(near(mixed), skip_stream_entering, feature_blend_scaling.reshape(1, -1))
    rows = exchange(copies, ROWS)
    out = call(
        mlp_kernel,
        shape((nrows, *own_tiles), bf16),
        [VMEM, HBM],
        [pltpu.VMEM(weights.shape, bf16), pltpu.SemaphoreType.DMA((2, *weights.shape[:2]))],
    )(near(rows), weights)
    out = exchange(out, ROWS)
    return call(final_kernel, jax.ShapeDtypeStruct((own_count, width), bf16), [VMEM] * 2)(near(out), near(own))


def solution(mesh):
    torus = Mesh(mesh.devices.reshape(4, 4, 4, 4, 2), SP + TP)
    placed = (
        P(SP + TP, None),
        P(SP, TP),
        P(SP, TP),
        P(SP, TP),
        P(SP, TP),
        P(TP, SP),
        P(TP, SP),
        P(TP),
        P(None, TP),
        P(None, TP),
        P(None, TP),
        P(TP),
        P(TP),
        P(TP, None),
        P(),
        P(SP, TP),
        P(TP, SP),
    )
    return jax.shard_map(layer, mesh=torus, in_specs=placed, out_specs=P(SP + TP, None), check_vma=False)
```

```python
import jax
import jax.numpy as jnp
from jax import lax
from jax.experimental import pallas as pl
from jax.experimental.pallas import tpu as pltpu
from jax.sharding import Mesh
from jax.sharding import PartitionSpec as P

HEADS = 8
HEAD_DIM = 64
STATE = 128
BLOCK = 128
WIDTH = HEADS * HEAD_DIM
RIM = 8
PAIR = 2 * HEAD_DIM
TAIL = 16
SP = ("zh", "zl", "y")
TP = ("x", "c")
ROWS = ("x", "y")
EPSILON = 1e-05
INTERPRET = False
ROOM = pltpu.CompilerParams(vmem_limit_bytes=16 << 20)

f32 = jnp.float32
bf16 = jnp.bfloat16
VMEM = pl.BlockSpec(memory_space=pltpu.VMEM)
SMEM = pl.BlockSpec(memory_space=pltpu.SMEM)
HBM = pl.BlockSpec(memory_space=pl.ANY)


def call(kernel, outs, in_specs, scratch=(), **kw):
    single = not isinstance(outs, (list, tuple))
    return pl.pallas_call(
        kernel,
        out_shape=outs,
        in_specs=in_specs,
        out_specs=VMEM if single else [VMEM] * len(outs),
        scratch_shapes=list(scratch),
        interpret=INTERPRET,
        **kw,
    )


def shape(dims, kind):
    return jax.ShapeDtypeStruct(dims, kind) if INTERPRET else pltpu.VMEM(dims, kind)


def near(value):
    return value if INTERPRET else pltpu.with_memory_space_constraint(value, pltpu.VMEM)


def exchange(value, axes):
    return lax.all_to_all(value, axes, split_axis=0, concat_axis=0, tiled=True)


def dot(a, b, dims, **kw):
    return lax.dot_general(a, b, (dims, ((), ())), preferred_element_type=f32, **kw)


def spread(rows, width):
    head = lax.broadcasted_iota(jnp.int32, (HEADS, HEADS * width), 0)
    lane = lax.broadcasted_iota(jnp.int32, (HEADS, HEADS * width), 1)
    chosen = jnp.where(lane // width == head, 1.0, 0.0).astype(f32)
    return dot(rows, chosen, ((0,), (0,)), precision=lax.Precision.HIGHEST)


def silu(value):
    return value / (1.0 + jnp.exp(-value))


def convolve(room, taps_ref, count):
    taps = taps_ref[...].astype(f32)
    width = taps.shape[0]
    total = None
    for k in range(width):
        start = RIM - width + 1 + k
        term = room[start : start + count, :] * taps[k : k + 1, :]
        total = term if total is None else total + term
    return total


def put_state(ref, place, start, state, logs):
    ref[place, start : start + PAIR, :] = state.astype(bf16)
    row = lax.broadcasted_iota(jnp.int32, (TAIL, STATE), 0)
    tail = jnp.zeros((TAIL, STATE), f32)
    for h in range(2):
        whole = jnp.broadcast_to(logs[h : h + 1, :], (TAIL, STATE))
        high = whole.astype(bf16).astype(f32)
        tail = jnp.where(row == 2 * h, high, jnp.where(row == 2 * h + 1, whole - high, tail))
    ref[place, start + PAIR : start + PAIR + TAIL, :] = tail.astype(bf16)


def take_state(ref, place, start):
    state = ref[place, start : start + PAIR, :].astype(f32)
    tail = ref[place, start + PAIR : start + PAIR + TAIL, :].astype(f32)
    return state, jnp.concatenate([tail[2 * h : 2 * h + 1, :] + tail[2 * h + 1 : 2 * h + 2, :] for h in range(2)], axis=0)


def factor(logs):
    grown = jnp.exp(logs)
    return jnp.concatenate([jnp.broadcast_to(grown[h : h + 1, :], (HEAD_DIM, STATE)) for h in range(2)], axis=0)


def first_kernel(x_ref, b_ref, c_ref, rim_ref):
    rim_ref[:, 0:WIDTH] = x_ref[...]
    rim_ref[:, WIDTH : WIDTH + STATE] = b_ref[...]
    rim_ref[:, WIDTH + STATE : WIDTH + 2 * STATE] = c_ref[...]


def early_kernel(
    x_ref, b_ref, c_ref, xt_ref, bt_ref, ct_ref, dt_ref, shrink_ref, speed_ref,
    x_out, b_out, c_out, cum_ref, weight_ref, mask_ref, x_room, b_room, c_room,
):
    for src_ref, taps_ref, out_ref, room in (
        (x_ref, xt_ref, x_out, x_room), (b_ref, bt_ref, b_out, b_room), (c_ref, ct_ref, c_out, c_room)
    ):
        room[0:RIM, :] = jnp.zeros((RIM, room.shape[1]), f32)
        room[RIM : RIM + BLOCK, :] = src_ref[...].astype(f32)
        out_ref[...] = convolve(room, taps_ref, BLOCK)
    before = dt_ref[...]
    steps = jnp.maximum(before, 0.0) + jnp.log1p(jnp.exp(-jnp.abs(before)))
    head = lax.broadcasted_iota(jnp.int32, (HEADS, BLOCK), 0)
    token = lax.broadcasted_iota(jnp.int32, (HEADS, BLOCK), 1)
    speed = jnp.zeros((HEADS, BLOCK), f32)
    for h in range(HEADS):
        speed = jnp.where(head == h, speed_ref[h], speed)
    cum = shrink_ref[...] - jnp.exp(speed) * steps
    reach = 1
    while reach < BLOCK:
        cum = cum + jnp.where(token >= reach, pltpu.roll(cum, reach, 1), 0.0)
        reach *= 2
    cum_ref[...] = cum
    weight_ref[...] = spread(steps * jnp.exp(cum[:, BLOCK - 1 : BLOCK] - cum), HEAD_DIM)
    columns = spread(cum, BLOCK)
    later = lax.broadcasted_iota(jnp.int32, (BLOCK, BLOCK), 0)
    earlier = lax.broadcasted_iota(jnp.int32, (BLOCK, BLOCK), 1)
    causal = later >= earlier
    for h in range(HEADS):
        away = columns[:, h * BLOCK : (h + 1) * BLOCK] - cum[h : h + 1, :]
        mask_ref[h] = jnp.exp(jnp.where(causal, away, -jnp.inf)) * steps[h : h + 1, :]


def local_kernel(
    x_ref, b_ref, c_ref, rim_ref, xt_ref, bt_ref, ct_ref, x_sum, b_sum, c_sum, cum_ref, weight_ref, mask_ref,
    up_ref, down_ref, skip_ref,
    pre_ref, query_ref, send_ref, x_room, b_room, c_room,
):
    rows = []
    lane = 0
    for src_ref, taps_ref, sum_ref, room in (
        (x_ref, xt_ref, x_sum, x_room), (b_ref, bt_ref, b_sum, b_room), (c_ref, ct_ref, c_sum, c_room)
    ):
        room[0:RIM, :] = rim_ref[:, lane : lane + room.shape[1]].astype(f32)
        room[RIM : 2 * RIM, :] = src_ref[...].astype(f32)
        lane += room.shape[1]
        head = convolve(room, taps_ref, RIM)
        rows.append(silu(jnp.concatenate([head, sum_ref[RIM:BLOCK, :]], axis=0)))
    values, keys, query = rows[0], rows[1].astype(bf16), rows[2].astype(bf16)
    query_ref[...] = query
    last = cum_ref[:, BLOCK - 1 : BLOCK]
    state = dot((values * weight_ref[...]).astype(bf16), keys, ((0,), (0,)))
    pieces = send_ref.shape[0]
    depth, units = up_ref.shape
    slabs = units // pieces // STATE
    for k in range(pieces):
        for j in range(slabs):
            lanes = slice((k * slabs + j) * STATE, (k * slabs + j + 1) * STATE)
            send_ref[k, j * depth : (j + 1) * depth, :] = up_ref[:, lanes]
            send_ref[k, (slabs + j) * depth : (slabs + j + 1) * depth, :] = down_ref[:, lanes]
        put_state(send_ref, k, 2 * slabs * depth, state[k * PAIR : (k + 1) * PAIR, :], last[2 * k : 2 * k + 2, :])
    scores = dot(query, keys, ((1,), (1,)))
    first = lax.broadcasted_iota(jnp.int32, (BLOCK, 2 * HEAD_DIM), 1) < HEAD_DIM
    for pair in range(HEADS // 2):
        lanes = slice(pair * 2 * HEAD_DIM, (pair + 1) * 2 * HEAD_DIM)
        two = values[:, lanes]
        two_low = two.astype(bf16)
        parts = []
        for h in (2 * pair, 2 * pair + 1):
            mixing = scores * mask_ref[h]
            parts.append(dot(mixing.astype(bf16), two_low, ((1,), (0,))))
        within = jnp.where(first, parts[0], parts[1])
        skip = jnp.where(first, skip_ref[2 * pair], skip_ref[2 * pair + 1])
        pre_ref[:, lanes] = within + skip * two


def row_kernel(got_ref, shard_ref, send_ref):
    start = shard_ref.shape[1]
    state = logs = None
    for k in range(got_ref.shape[0]):
        shard_ref[k] = got_ref[k, 0:start, :]
        more, step = take_state(got_ref, k, start)
        state, logs = (more, step) if state is None else (state * factor(step) + more, logs + step)
    for k in range(send_ref.shape[0]):
        put_state(send_ref, k, 0, state, logs)


def near_kernel(got_ref, send_ref, state_ref, logs_ref):
    here = lax.axis_index("zl")
    state = before = jnp.zeros((PAIR, STATE), f32)
    logs = passed = jnp.zeros((2, STATE), f32)
    for k in range(got_ref.shape[0]):
        more, step = take_state(got_ref, k, 0)
        state, logs = state * factor(step) + more, logs + step
        before, passed = jnp.where(k < here, state, before), jnp.where(k < here, logs, passed)
    state_ref[...] = before
    logs_ref[...] = passed
    for k in range(send_ref.shape[0]):
        put_state(send_ref, k, 0, state, logs)


def far_kernel(got_ref, state_ref, logs_ref, rows_ref, out_ref):
    here = lax.axis_index("zh")
    state = before = jnp.zeros((PAIR, STATE), f32)
    for k in range(got_ref.shape[0] - 1):
        more, step = take_state(got_ref, k, 0)
        state = state * factor(step) + more
        before = jnp.where(k < here, state, before)
    state = before * factor(logs_ref[...]) + state_ref[...]
    start = rows_ref.shape[1] - PAIR - TAIL
    for k in range(rows_ref.shape[0]):
        out_ref[k] = state.astype(bf16)
        if k + 1 < rows_ref.shape[0]:
            more, step = take_state(rows_ref, k, start)
            state = state * factor(step) + more


def gate_kernel(pre_ref, query_ref, cum_ref, inc_ref, gate_ref, gain_ref, w_ref, out_ref):
    inc = inc_ref[...].reshape(WIDTH, STATE)
    arriving = dot(query_ref[...], inc, ((1,), (1,))) * spread(jnp.exp(cum_ref[...]), HEAD_DIM)
    gated = (pre_ref[...] + arriving) * silu(gate_ref[...].astype(f32))
    scale = lax.rsqrt(jnp.mean(gated * gated, axis=-1, keepdims=True) + EPSILON)
    heads_out = (gated * scale * gain_ref[...]).astype(bf16)
    out = dot(heads_out, w_ref[...], ((1,), (0,)))
    out_ref[...] = out.astype(bf16).reshape(out_ref.shape)


def norm_kernel(got_ref, skip_ref, gain_ref, own_ref, copies_ref):
    total = got_ref[0].astype(f32)
    for k in range(1, got_ref.shape[0]):
        total = total + got_ref[k].astype(f32)
    total = total.reshape(own_ref.shape)
    own = (skip_ref[...].astype(f32) + total.astype(bf16).astype(f32)).astype(bf16)
    own_ref[...] = own
    wide = own.astype(f32)
    scale = lax.rsqrt(jnp.mean(wide * wide, axis=-1, keepdims=True) + EPSILON)
    normed = (wide * scale * gain_ref[...]).astype(bf16)
    for k in range(copies_ref.shape[0]):
        copies_ref[k] = normed.reshape(copies_ref.shape[1:])


def mlp_kernel(rows_ref, w_ref, out_ref, w_room, sems):
    halves, shards, inner, slabs, each_depth, lanes = w_ref.shape
    pieces = sems.shape[2]
    take = shards // pieces
    size = take * inner * each_depth
    copies = []
    for part in range(2):
        some = pl.ds(part * (slabs // 2), slabs // 2)
        for j in range(pieces):
            for k in range(halves):
                place = (k, pl.ds(j * take, take), slice(None), some)
                copies.append(pltpu.make_async_copy(w_ref.at[place], w_room.at[place], sems.at[part, k, j]))
    count = pieces * halves
    for copy in copies[:count]:
        copy.start()

    def piece(k, j, first):
        parts = [w_room[k, j * take : (j + 1) * take, :, n, :, :] for n in (first, first + 1)]
        return jnp.concatenate([p.reshape(size, lanes) for p in parts], axis=1)

    depth = rows_ref.shape[-1]
    rows = rows_ref[...].reshape(-1, depth)
    lifted = [None] * halves
    for j in range(pieces):
        for k in range(halves):
            copies[j * halves + k].wait()
            copies[count + j * halves + k].start()
            part = dot(rows[:, j * size : (j + 1) * size], piece(k, j, 0), ((1,), (0,)))
            lifted[k] = part if lifted[k] is None else lifted[k] + part
    hidden = []
    for k in range(halves):
        up = jnp.maximum(lifted[k], 0.0)
        hidden.append((up * up).astype(bf16))
    for j in range(pieces):
        total = None
        for k in range(halves):
            copies[count + j * halves + k].wait()
            part = dot(hidden[k], piece(k, j, slabs // 2), ((1,), (1,)))
            total = part if total is None else total + part
        out_ref[:, :, :, j * size : (j + 1) * size] = total.astype(bf16).reshape(*out_ref.shape[:3], size)


def final_kernel(got_ref, own_ref, out_ref):
    total = got_ref[0].astype(f32)
    for k in range(1, got_ref.shape[0]):
        total = total + got_ref[k].astype(f32)
    total = total.reshape(own_ref.shape)
    out_ref[...] = (own_ref[...].astype(f32) + total.astype(bf16).astype(f32)).astype(bf16)


def layer(
    skip_stream_entering,
    content_signal_matrix,
    writer_signal_matrix,
    reader_signal_matrix,
    multiplier_signal,
    interval_before_softplus,
    extra_log_shrink,
    log_forget_speed,
    content_filter_coefs,
    writer_filter_coefs,
    reader_filter_coefs,
    skip_path_factor,
    cluster_scaling_vector,
    blend_result_matrix,
    feature_blend_scaling,
    widening_matrix,
    narrowing_matrix,
):
    ny, nzl, nzh = (lax.axis_size(name) for name in ("y", "zl", "zh"))
    nsp = nzh * nzl * ny
    ntp = lax.axis_size("x") * lax.axis_size("c")
    nrows = ny * lax.axis_size("x")
    own_count, width = skip_stream_entering.shape
    own_tiles = (own_count // 8, 8, width)
    depth, units = widening_matrix.shape
    shard = 2 * depth * units // ny // STATE

    rim = pl.pallas_call(
        first_kernel,
        grid=(1,),
        out_shape=shape((RIM, WIDTH + 2 * STATE), bf16),
        in_specs=[pl.BlockSpec((RIM, n), lambda i: (BLOCK // RIM - 1, 0)) for n in (WIDTH, STATE, STATE)],
        out_specs=pl.BlockSpec((RIM, WIDTH + 2 * STATE), lambda i: (0, 0)),
        interpret=INTERPRET,
        compiler_params=pltpu.CompilerParams(vmem_limit_bytes=54 << 20),
    )(content_signal_matrix, writer_signal_matrix, reader_signal_matrix)
    rim = lax.ppermute(rim, SP, [(k, k + 1) for k in range(nsp - 1)])
    *sums, cum, weight, mask = call(
        early_kernel,
        [
            shape((BLOCK, WIDTH), f32),
            shape((BLOCK, STATE), f32),
            shape((BLOCK, STATE), f32),
            shape((HEADS, BLOCK), f32),
            shape((BLOCK, WIDTH), f32),
            shape((HEADS, BLOCK, BLOCK), f32),
        ],
        [VMEM] * 8 + [SMEM],
        [pltpu.VMEM((RIM + BLOCK, n), f32) for n in (WIDTH, STATE, STATE)],
        compiler_params=pltpu.CompilerParams(vmem_limit_bytes=54 << 20),
    )(
        content_signal_matrix,
        writer_signal_matrix,
        reader_signal_matrix,
        content_filter_coefs,
        writer_filter_coefs,
        reader_filter_coefs,
        interval_before_softplus,
        extra_log_shrink,
        log_forget_speed,
    )

    def whole(value):
        zeros = (0,) * value.ndim
        return pl.BlockSpec(value.shape, lambda i: zeros)

    head_rows = (content_signal_matrix, writer_signal_matrix, reader_signal_matrix)
    taps = (content_filter_coefs, writer_filter_coefs, reader_filter_coefs)
    kept = [near(value) for value in (*sums, cum, weight, mask)]
    outs = [
        shape((BLOCK, WIDTH), f32),
        shape((BLOCK, STATE), bf16),
        shape((ny, shard + PAIR + TAIL, STATE), bf16),
    ]
    narrowing = narrowing_matrix.T
    pre, query, send = pl.pallas_call(
        local_kernel,
        grid=(1,),
        out_shape=outs,
        in_specs=[pl.BlockSpec((RIM, value.shape[1]), lambda i: (0, 0)) for value in head_rows]
        + [VMEM]
        + [whole(value) for value in taps]
        + [VMEM] * len(kept)
        + [whole(widening_matrix), whole(narrowing), SMEM],
        out_specs=[VMEM] * 3,
        scratch_shapes=[pltpu.VMEM((2 * RIM, n), f32) for n in (WIDTH, STATE, STATE)],
        interpret=INTERPRET,
        compiler_params=pltpu.CompilerParams(vmem_limit_bytes=54 << 20),
    )(*head_rows, near(rim), *taps, *kept, widening_matrix, narrowing, skip_path_factor)
    rows = near(exchange(send, "y"))
    parts, send = call(
        row_kernel,
        [jax.ShapeDtypeStruct((ny, shard, STATE), bf16), shape((nzl, PAIR + TAIL, STATE), bf16)],
        [VMEM],
        compiler_params=ROOM,
    )(rows)
    weights = lax.all_gather(parts.reshape(ny * shard, STATE), ("c", "zh", "zl"), axis=0, tiled=True)
    weights = weights.reshape(-1, nzh * nzl, ny, shard // depth, depth, STATE)
    got = near(exchange(send, "zl"))
    send, state, logs = call(
        near_kernel,
        [shape((nzh, PAIR + TAIL, STATE), bf16), shape((PAIR, STATE), f32), shape((2, STATE), f32)],
        [VMEM],
        compiler_params=ROOM,
    )(got)
    got = near(exchange(send, "zh"))
    before = call(far_kernel, shape((ny, PAIR, STATE), bf16), [VMEM] * 4, compiler_params=ROOM)(
        got, near(state), near(logs), rows
    )
    incoming = exchange(before, "y")
    mixed = call(
        gate_kernel,
        shape((ntp, *own_tiles), bf16),
        [VMEM] * 7,
        compiler_params=ROOM,
    )(
        near(pre),
        near(query),
        near(cum),
        near(incoming),
        multiplier_signal,
        cluster_scaling_vector.reshape(1, -1),
        near(blend_result_matrix),
    )
    mixed = exchange(mixed, TP)
    own, copies = call(
        norm_kernel,
        [shape((own_count, width), bf16), shape((nrows, *own_tiles), bf16)],
        [VMEM] * 3,
    )(near(mixed), skip_stream_entering, feature_blend_scaling.reshape(1, -1))
    rows = exchange(copies, ROWS)
    out = call(
        mlp_kernel,
        shape((nrows, *own_tiles), bf16),
        [VMEM, HBM],
        [pltpu.VMEM(weights.shape, bf16), pltpu.SemaphoreType.DMA((2, weights.shape[0], 4))],
    )(near(rows), weights)
    out = exchange(out, ROWS)
    return call(final_kernel, jax.ShapeDtypeStruct((own_count, width), bf16), [VMEM] * 2)(near(out), near(own))


def solution(mesh):
    torus = Mesh(mesh.devices.reshape(4, 4, 4, 4, 2), SP + TP)
    placed = (
        P(SP + TP, None),
        P(SP, TP),
        P(SP, TP),
        P(SP, TP),
        P(SP, TP),
        P(TP, SP),
        P(TP, SP),
        P(TP),
        P(None, TP),
        P(None, TP),
        P(None, TP),
        P(TP),
        P(TP),
        P(TP, None),
        P(),
        P(SP, TP),
        P(TP, SP),
    )
    return jax.shard_map(layer, mesh=torus, in_specs=placed, out_specs=P(SP + TP, None), check_vma=False)
```

```python
import jax
import jax.numpy as jnp
from jax import lax
from jax.experimental import pallas as pl
from jax.experimental.pallas import tpu as pltpu
from jax.sharding import Mesh
from jax.sharding import PartitionSpec as P

HEADS = 8
HEAD_DIM = 64
STATE = 128
BLOCK = 128
WIDTH = HEADS * HEAD_DIM
RIM = 8
PAIR = 2 * HEAD_DIM
TAIL = 16
SP = ("zh", "zl", "y")
TP = ("x", "c")
ROWS = ("x", "y")
EPSILON = 1e-05
INTERPRET = False
ROOM = pltpu.CompilerParams(vmem_limit_bytes=16 << 20)

f32 = jnp.float32
bf16 = jnp.bfloat16
VMEM = pl.BlockSpec(memory_space=pltpu.VMEM)
SMEM = pl.BlockSpec(memory_space=pltpu.SMEM)
HBM = pl.BlockSpec(memory_space=pl.ANY)


def call(kernel, outs, in_specs, scratch=(), **kw):
    single = not isinstance(outs, (list, tuple))
    return pl.pallas_call(
        kernel,
        out_shape=outs,
        in_specs=in_specs,
        out_specs=VMEM if single else [VMEM] * len(outs),
        scratch_shapes=list(scratch),
        interpret=INTERPRET,
        **kw,
    )


def shape(dims, kind):
    return jax.ShapeDtypeStruct(dims, kind) if INTERPRET else pltpu.VMEM(dims, kind)


def near(value):
    return value if INTERPRET else pltpu.with_memory_space_constraint(value, pltpu.VMEM)


def exchange(value, axes):
    return lax.all_to_all(value, axes, split_axis=0, concat_axis=0, tiled=True)


def dot(a, b, dims, **kw):
    return lax.dot_general(a, b, (dims, ((), ())), preferred_element_type=f32, **kw)


def spread(rows, width):
    head = lax.broadcasted_iota(jnp.int32, (HEADS, HEADS * width), 0)
    lane = lax.broadcasted_iota(jnp.int32, (HEADS, HEADS * width), 1)
    chosen = jnp.where(lane // width == head, 1.0, 0.0).astype(f32)
    return dot(rows, chosen, ((0,), (0,)), precision=lax.Precision.HIGHEST)


def silu(value):
    return value / (1.0 + jnp.exp(-value))


def convolve(room, taps_ref, count):
    taps = taps_ref[...].astype(f32)
    width = taps.shape[0]
    total = None
    for k in range(width):
        start = RIM - width + 1 + k
        term = room[start : start + count, :] * taps[k : k + 1, :]
        total = term if total is None else total + term
    return total


def put_state(ref, place, start, state, logs):
    ref[place, start : start + PAIR, :] = state.astype(bf16)
    row = lax.broadcasted_iota(jnp.int32, (TAIL, STATE), 0)
    tail = jnp.zeros((TAIL, STATE), f32)
    for h in range(2):
        whole = jnp.broadcast_to(logs[h : h + 1, :], (TAIL, STATE))
        high = whole.astype(bf16).astype(f32)
        tail = jnp.where(row == 2 * h, high, jnp.where(row == 2 * h + 1, whole - high, tail))
    ref[place, start + PAIR : start + PAIR + TAIL, :] = tail.astype(bf16)


def take_state(ref, place, start):
    state = ref[place, start : start + PAIR, :].astype(f32)
    tail = ref[place, start + PAIR : start + PAIR + TAIL, :].astype(f32)
    return state, jnp.concatenate([tail[2 * h : 2 * h + 1, :] + tail[2 * h + 1 : 2 * h + 2, :] for h in range(2)], axis=0)


def factor(logs):
    grown = jnp.exp(logs)
    return jnp.concatenate([jnp.broadcast_to(grown[h : h + 1, :], (HEAD_DIM, STATE)) for h in range(2)], axis=0)


def first_kernel(x_ref, b_ref, c_ref, rim_ref):
    rim_ref[:, 0:WIDTH] = x_ref[...]
    rim_ref[:, WIDTH : WIDTH + STATE] = b_ref[...]
    rim_ref[:, WIDTH + STATE : WIDTH + 2 * STATE] = c_ref[...]


def early_kernel(
    x_ref, b_ref, c_ref, xt_ref, bt_ref, ct_ref, dt_ref, shrink_ref, speed_ref,
    x_out, b_out, c_out, cum_ref, weight_ref, mask_ref, x_room, b_room, c_room,
):
    for src_ref, taps_ref, out_ref, room in (
        (x_ref, xt_ref, x_out, x_room), (b_ref, bt_ref, b_out, b_room), (c_ref, ct_ref, c_out, c_room)
    ):
        room[0:RIM, :] = jnp.zeros((RIM, room.shape[1]), f32)
        room[RIM : RIM + BLOCK, :] = src_ref[...].astype(f32)
        out_ref[...] = convolve(room, taps_ref, BLOCK)
    before = dt_ref[...]
    steps = jnp.maximum(before, 0.0) + jnp.log1p(jnp.exp(-jnp.abs(before)))
    head = lax.broadcasted_iota(jnp.int32, (HEADS, BLOCK), 0)
    token = lax.broadcasted_iota(jnp.int32, (HEADS, BLOCK), 1)
    speed = jnp.zeros((HEADS, BLOCK), f32)
    for h in range(HEADS):
        speed = jnp.where(head == h, speed_ref[h], speed)
    cum = shrink_ref[...] - jnp.exp(speed) * steps
    reach = 1
    while reach < BLOCK:
        cum = cum + jnp.where(token >= reach, pltpu.roll(cum, reach, 1), 0.0)
        reach *= 2
    cum_ref[...] = cum
    weight_ref[...] = spread(steps * jnp.exp(cum[:, BLOCK - 1 : BLOCK] - cum), HEAD_DIM)
    columns = spread(cum, BLOCK)
    later = lax.broadcasted_iota(jnp.int32, (BLOCK, BLOCK), 0)
    earlier = lax.broadcasted_iota(jnp.int32, (BLOCK, BLOCK), 1)
    causal = later >= earlier
    for h in range(HEADS):
        away = columns[:, h * BLOCK : (h + 1) * BLOCK] - cum[h : h + 1, :]
        mask_ref[h] = jnp.exp(jnp.where(causal, away, -jnp.inf)) * steps[h : h + 1, :]


def local_kernel(
    x_ref, b_ref, c_ref, rim_ref, xt_ref, bt_ref, ct_ref, x_sum, b_sum, c_sum, cum_ref, weight_ref, mask_ref,
    up_ref, down_ref, skip_ref,
    pre_ref, query_ref, send_ref, x_room, b_room, c_room,
):
    rows = []
    lane = 0
    for src_ref, taps_ref, sum_ref, room in (
        (x_ref, xt_ref, x_sum, x_room), (b_ref, bt_ref, b_sum, b_room), (c_ref, ct_ref, c_sum, c_room)
    ):
        room[0:RIM, :] = rim_ref[:, lane : lane + room.shape[1]].astype(f32)
        room[RIM : 2 * RIM, :] = src_ref[...].astype(f32)
        lane += room.shape[1]
        head = convolve(room, taps_ref, RIM)
        rows.append(silu(jnp.concatenate([head, sum_ref[RIM:BLOCK, :]], axis=0)))
    values, keys, query = rows[0], rows[1].astype(bf16), rows[2].astype(bf16)
    query_ref[...] = query
    last = cum_ref[:, BLOCK - 1 : BLOCK]
    state = dot((values * weight_ref[...]).astype(bf16), keys, ((0,), (0,)))
    pieces = send_ref.shape[0]
    depth, units = up_ref.shape
    slabs = units // pieces // STATE
    for k in range(pieces):
        for j in range(slabs):
            lanes = slice((k * slabs + j) * STATE, (k * slabs + j + 1) * STATE)
            send_ref[k, j * depth : (j + 1) * depth, :] = up_ref[:, lanes]
            send_ref[k, (slabs + j) * depth : (slabs + j + 1) * depth, :] = down_ref[:, lanes]
        put_state(send_ref, k, 2 * slabs * depth, state[k * PAIR : (k + 1) * PAIR, :], last[2 * k : 2 * k + 2, :])
    scores = dot(query, keys, ((1,), (1,)))
    first = lax.broadcasted_iota(jnp.int32, (BLOCK, 2 * HEAD_DIM), 1) < HEAD_DIM
    for pair in range(HEADS // 2):
        lanes = slice(pair * 2 * HEAD_DIM, (pair + 1) * 2 * HEAD_DIM)
        two = values[:, lanes]
        two_low = two.astype(bf16)
        parts = []
        for h in (2 * pair, 2 * pair + 1):
            mixing = scores * mask_ref[h]
            parts.append(dot(mixing.astype(bf16), two_low, ((1,), (0,))))
        within = jnp.where(first, parts[0], parts[1])
        skip = jnp.where(first, skip_ref[2 * pair], skip_ref[2 * pair + 1])
        pre_ref[:, lanes] = within + skip * two


def row_kernel(got_ref, shard_ref, send_ref):
    start = shard_ref.shape[1]
    state = logs = None
    for k in range(got_ref.shape[0]):
        shard_ref[k] = got_ref[k, 0:start, :]
        more, step = take_state(got_ref, k, start)
        state, logs = (more, step) if state is None else (state * factor(step) + more, logs + step)
    for k in range(send_ref.shape[0]):
        put_state(send_ref, k, 0, state, logs)


def near_kernel(got_ref, send_ref, state_ref, logs_ref):
    here = lax.axis_index("zl")
    state = before = jnp.zeros((PAIR, STATE), f32)
    logs = passed = jnp.zeros((2, STATE), f32)
    for k in range(got_ref.shape[0]):
        more, step = take_state(got_ref, k, 0)
        state, logs = state * factor(step) + more, logs + step
        before, passed = jnp.where(k < here, state, before), jnp.where(k < here, logs, passed)
    state_ref[...] = before
    logs_ref[...] = passed
    for k in range(send_ref.shape[0]):
        put_state(send_ref, k, 0, state, logs)


def far_kernel(got_ref, state_ref, logs_ref, rows_ref, out_ref):
    here = lax.axis_index("zh")
    state = before = jnp.zeros((PAIR, STATE), f32)
    for k in range(got_ref.shape[0] - 1):
        more, step = take_state(got_ref, k, 0)
        state = state * factor(step) + more
        before = jnp.where(k < here, state, before)
    state = before * factor(logs_ref[...]) + state_ref[...]
    start = rows_ref.shape[1] - PAIR - TAIL
    for k in range(rows_ref.shape[0]):
        out_ref[k] = state.astype(bf16)
        if k + 1 < rows_ref.shape[0]:
            more, step = take_state(rows_ref, k, start)
            state = state * factor(step) + more


def gate_kernel(pre_ref, query_ref, cum_ref, inc_ref, gate_ref, gain_ref, w_ref, out_ref):
    inc = inc_ref[...].reshape(WIDTH, STATE)
    arriving = dot(query_ref[...], inc, ((1,), (1,))) * spread(jnp.exp(cum_ref[...]), HEAD_DIM)
    gated = (pre_ref[...] + arriving) * silu(gate_ref[...].astype(f32))
    scale = lax.rsqrt(jnp.mean(gated * gated, axis=-1, keepdims=True) + EPSILON)
    heads_out = (gated * scale * gain_ref[...]).astype(bf16)
    out = dot(heads_out, w_ref[...], ((1,), (0,)))
    out_ref[...] = out.astype(bf16).reshape(out_ref.shape)


def norm_kernel(got_ref, skip_ref, gain_ref, own_ref, copies_ref):
    total = got_ref[0].astype(f32)
    for k in range(1, got_ref.shape[0]):
        total = total + got_ref[k].astype(f32)
    total = total.reshape(own_ref.shape)
    own = (skip_ref[...].astype(f32) + total.astype(bf16).astype(f32)).astype(bf16)
    own_ref[...] = own
    wide = own.astype(f32)
    scale = lax.rsqrt(jnp.mean(wide * wide, axis=-1, keepdims=True) + EPSILON)
    normed = (wide * scale * gain_ref[...]).astype(bf16)
    for k in range(copies_ref.shape[0]):
        copies_ref[k] = normed.reshape(copies_ref.shape[1:])


def mlp_kernel(rows_ref, w_ref, out_ref, w_room, sems):
    halves, shards, inner, slabs, each_depth, lanes = w_ref.shape
    pieces = sems.shape[1]
    take = shards // pieces
    size = take * inner * each_depth
    copies = []
    for j in range(pieces):
        for k in range(halves):
            part = pl.ds(j * take, take)
            copy = pltpu.make_async_copy(w_ref.at[k, part], w_room.at[k, part], sems.at[k, j])
            copy.start()
            copies.append(copy)

    def piece(k, j, first):
        parts = [w_room[k, j * take : (j + 1) * take, :, n, :, :] for n in (first, first + 1)]
        return jnp.concatenate([p.reshape(size, lanes) for p in parts], axis=1)

    depth = rows_ref.shape[-1]
    rows = rows_ref[...].reshape(-1, depth)
    lifted = [None] * halves
    for j in range(pieces):
        for k in range(halves):
            copies[j * halves + k].wait()
            part = dot(rows[:, j * size : (j + 1) * size], piece(k, j, 0), ((1,), (0,)))
            lifted[k] = part if lifted[k] is None else lifted[k] + part
    hidden = []
    for k in range(halves):
        up = jnp.maximum(lifted[k], 0.0)
        hidden.append((up * up).astype(bf16))
    for j in range(pieces):
        total = None
        for k in range(halves):
            part = dot(hidden[k], piece(k, j, slabs // 2), ((1,), (1,)))
            total = part if total is None else total + part
        out_ref[:, :, :, j * size : (j + 1) * size] = total.astype(bf16).reshape(*out_ref.shape[:3], size)


def final_kernel(got_ref, own_ref, out_ref):
    total = got_ref[0].astype(f32)
    for k in range(1, got_ref.shape[0]):
        total = total + got_ref[k].astype(f32)
    total = total.reshape(own_ref.shape)
    out_ref[...] = (own_ref[...].astype(f32) + total.astype(bf16).astype(f32)).astype(bf16)


def layer(
    skip_stream_entering,
    content_signal_matrix,
    writer_signal_matrix,
    reader_signal_matrix,
    multiplier_signal,
    interval_before_softplus,
    extra_log_shrink,
    log_forget_speed,
    content_filter_coefs,
    writer_filter_coefs,
    reader_filter_coefs,
    skip_path_factor,
    cluster_scaling_vector,
    blend_result_matrix,
    feature_blend_scaling,
    widening_matrix,
    narrowing_matrix,
):
    ny, nzl, nzh = (lax.axis_size(name) for name in ("y", "zl", "zh"))
    nsp = nzh * nzl * ny
    ntp = lax.axis_size("x") * lax.axis_size("c")
    nrows = ny * lax.axis_size("x")
    own_count, width = skip_stream_entering.shape
    own_tiles = (own_count // 8, 8, width)
    depth, units = widening_matrix.shape
    shard = 2 * depth * units // ny // STATE

    rim = pl.pallas_call(
        first_kernel,
        grid=(1,),
        out_shape=shape((RIM, WIDTH + 2 * STATE), bf16),
        in_specs=[pl.BlockSpec((RIM, n), lambda i: (BLOCK // RIM - 1, 0)) for n in (WIDTH, STATE, STATE)],
        out_specs=pl.BlockSpec((RIM, WIDTH + 2 * STATE), lambda i: (0, 0)),
        interpret=INTERPRET,
        compiler_params=pltpu.CompilerParams(vmem_limit_bytes=54 << 20),
    )(content_signal_matrix, writer_signal_matrix, reader_signal_matrix)
    rim = lax.ppermute(rim, SP, [(k, k + 1) for k in range(nsp - 1)])
    *sums, cum, weight, mask = call(
        early_kernel,
        [
            shape((BLOCK, WIDTH), f32),
            shape((BLOCK, STATE), f32),
            shape((BLOCK, STATE), f32),
            shape((HEADS, BLOCK), f32),
            shape((BLOCK, WIDTH), f32),
            shape((HEADS, BLOCK, BLOCK), f32),
        ],
        [VMEM] * 8 + [SMEM],
        [pltpu.VMEM((RIM + BLOCK, n), f32) for n in (WIDTH, STATE, STATE)],
        compiler_params=pltpu.CompilerParams(vmem_limit_bytes=54 << 20),
    )(
        content_signal_matrix,
        writer_signal_matrix,
        reader_signal_matrix,
        content_filter_coefs,
        writer_filter_coefs,
        reader_filter_coefs,
        interval_before_softplus,
        extra_log_shrink,
        log_forget_speed,
    )

    def whole(value):
        zeros = (0,) * value.ndim
        return pl.BlockSpec(value.shape, lambda i: zeros)

    head_rows = (content_signal_matrix, writer_signal_matrix, reader_signal_matrix)
    taps = (content_filter_coefs, writer_filter_coefs, reader_filter_coefs)
    kept = [near(value) for value in (*sums, cum, weight, mask)]
    outs = [
        shape((BLOCK, WIDTH), f32),
        shape((BLOCK, STATE), bf16),
        shape((ny, shard + PAIR + TAIL, STATE), bf16),
    ]
    narrowing = narrowing_matrix.T
    pre, query, send = pl.pallas_call(
        local_kernel,
        grid=(1,),
        out_shape=outs,
        in_specs=[pl.BlockSpec((RIM, value.shape[1]), lambda i: (0, 0)) for value in head_rows]
        + [VMEM]
        + [whole(value) for value in taps]
        + [VMEM] * len(kept)
        + [whole(widening_matrix), whole(narrowing), SMEM],
        out_specs=[VMEM] * 3,
        scratch_shapes=[pltpu.VMEM((2 * RIM, n), f32) for n in (WIDTH, STATE, STATE)],
        interpret=INTERPRET,
        compiler_params=pltpu.CompilerParams(vmem_limit_bytes=54 << 20),
    )(*head_rows, near(rim), *taps, *kept, widening_matrix, narrowing, skip_path_factor)
    rows = near(exchange(send, "y"))
    parts, send = call(
        row_kernel,
        [jax.ShapeDtypeStruct((ny, shard, STATE), bf16), shape((nzl, PAIR + TAIL, STATE), bf16)],
        [VMEM],
        compiler_params=ROOM,
    )(rows)
    weights = lax.all_gather(parts.reshape(ny * shard, STATE), ("c", "zh", "zl"), axis=0, tiled=True)
    weights = weights.reshape(-1, nzh * nzl, ny, shard // depth, depth, STATE)
    got = near(exchange(send, "zl"))
    send, state, logs = call(
        near_kernel,
        [shape((nzh, PAIR + TAIL, STATE), bf16), shape((PAIR, STATE), f32), shape((2, STATE), f32)],
        [VMEM],
        compiler_params=ROOM,
    )(got)
    got = near(exchange(send, "zh"))
    before = call(far_kernel, shape((ny, PAIR, STATE), bf16), [VMEM] * 4, compiler_params=ROOM)(
        got, near(state), near(logs), rows
    )
    incoming = exchange(before, "y")
    mixed = call(
        gate_kernel,
        shape((ntp, *own_tiles), bf16),
        [VMEM] * 7,
        compiler_params=ROOM,
    )(
        near(pre),
        near(query),
        near(cum),
        near(incoming),
        multiplier_signal,
        cluster_scaling_vector.reshape(1, -1),
        near(blend_result_matrix),
    )
    mixed = exchange(mixed, TP)
    own, copies = call(
        norm_kernel,
        [shape((own_count, width), bf16), shape((nrows, *own_tiles), bf16)],
        [VMEM] * 3,
        compiler_params=ROOM,
    )(near(mixed), skip_stream_entering, feature_blend_scaling.reshape(1, -1))
    rows = exchange(copies, ROWS)
    out = call(
        mlp_kernel,
        shape((nrows, *own_tiles), bf16),
        [VMEM, HBM],
        [pltpu.VMEM(weights.shape, bf16), pltpu.SemaphoreType.DMA((weights.shape[0], 4))],
    )(near(rows), weights)
    out = exchange(out, ROWS)
    return call(final_kernel, jax.ShapeDtypeStruct((own_count, width), bf16), [VMEM] * 2)(near(out), near(own))


def solution(mesh):
    torus = Mesh(mesh.devices.reshape(4, 4, 4, 4, 2), SP + TP)
    placed = (
        P(SP + TP, None),
        P(SP, TP),
        P(SP, TP),
        P(SP, TP),
        P(SP, TP),
        P(TP, SP),
        P(TP, SP),
        P(TP),
        P(None, TP),
        P(None, TP),
        P(None, TP),
        P(TP),
        P(TP),
        P(TP, None),
        P(),
        P(SP, TP),
        P(TP, SP),
    )
    return jax.shard_map(layer, mesh=torus, in_specs=placed, out_specs=P(SP + TP, None), check_vma=False)
```
